512 devices in a mesh: grp: 2 (over y), ep: 16 (over z), tp: 16 (over x, core).
Axes of the slice: x: 8, y: 2, z: 16, core: 2. Of those that a mesh axis runs over, the one named last changes fastest.
The devices are a block of a 8x16x16 slice.
Arguments:
- tokens: bfloat16 [192, 2048], P('grp', 'ep'), parts along dimension 0, may hold values from -70 to 70
- first_gain: float32 [2048], replicated, may hold values from 0.1 to 1.9
- w_query: bfloat16 [2048, 2048], P('ep', 'tp'), may hold values from -0.125 to 0.125
- w_key: bfloat16 [2048, 2048], P('ep', 'tp'), may hold values from -0.125 to 0.125
- w_value: bfloat16 [2048, 4096], P('ep', 'tp'), may hold values from -0.125 to 0.125
- w_outgate: bfloat16 [2048, 4096], P('ep', 'tp'), may hold values from -0.125 to 0.125
- w_input: bfloat16 [2048, 16], replicated, may hold values from -0.125 to 0.125
- w_forget: bfloat16 [2048, 16], replicated, may hold values from -0.125 to 0.125
- input_bias: float32 [16], replicated, may hold values from -3 to 3
- forget_bias: float32 [16], replicated, may hold values from -2 to 5
- head_gain: float32 [4096], replicated, may hold values from 0.1 to 1.9
- w_project: bfloat16 [4096, 2048], P('tp', 'ep'), may hold values from -0.09375 to 0.09375
- cell_state: float32 [192, 16, 128, 256], P(('grp', 'ep'), 'tp'), parts along dimension 0, may hold values from -6 to 6
- norm_state: float32 [192, 16, 128], P(('grp', 'ep'), 'tp'), parts along dimension 0, may hold values from -6 to 6
- max_state: float32 [192, 16], P(('grp', 'ep'), 'tp'), parts along dimension 0, may hold values from -110 to 110
- second_gain: float32 [2048], replicated, may hold values from 0.1 to 1.9
- routes: int32 [192, 2], P('grp'), parts along dimension 0, may hold values from 0 to 15, all different within a row; in each aligned block of 6 rows (0 to 5, 6 to 11, ...) at most 2 rows name the same one
- route_weight: float32 [192, 2], P('grp'), parts along dimension 0, may hold values from 0.2 to 1
- expert_gate: bfloat16 [16, 2048, 4096], P('ep', None, 'tp'), may hold values from -0.125 to 0.125
- expert_up: bfloat16 [16, 2048, 4096], P('ep', None, 'tp'), may hold values from -0.125 to 0.125
- expert_down: bfloat16 [16, 4096, 2048], P('ep', 'tp'), may hold values from -0.09375 to 0.09375
Outputs:
- layer_out: bfloat16 [192, 2048], P('grp', 'ep'), parts along dimension 0
- new_cell: float32 [192, 16, 128, 256], P(('grp', 'ep'), 'tp'), parts along dimension 0
- new_norm: float32 [192, 16, 128], P(('grp', 'ep'), 'tp'), parts along dimension 0
- new_max: float32 [192, 16], P(('grp', 'ep'), 'tp'), parts along dimension 0
The draws below stay inside these ranges and needn't reach their ends.
There are 2 independent parts, one for each index of `grp`. The reference program is written for one: setup_inputs(seed, part) draws one part's arguments, and reference() takes and returns one part's arrays. A program takes and returns all parts, laid end to end along the dimension named above; an argument that names none is the same for every part. Nothing has to cross between parts.
Inputs may be any that keep to these rules, and one draw needn't show every extreme that they name: `routes`: each sequence names 2 different experts. In each aligned block of 6 sequences no expert is named by more than 2 of them, a bound that some block reaches.
All inputs are finite; a program needn't handle non-finite values.
Results may differ from the reference program's by a relative error of at most 0.0065.
Values may be sent and summed in bfloat16 or wider, within the bound.
A program may use at most 64 MiB of HBM per device.

```python
import math
import jax
import jax.numpy as jnp
import numpy as np
from jax import lax

D = 2048
HEADS = 16
DK = 128
DV = 256
FF = 4096
TOP = 2
SEQ_DEV = 6
EXPERTS = 16
SEQS = 96
CAP = 2
N_EP = 16


def draw_tokens(key, part):
    key_base, key_cols = jax.random.split(key, 2)
    position = jnp.arange(D, dtype=jnp.float32) / D
    drawn = jnp.clip(jax.random.normal(key_base, (SEQS, D), jnp.float32), -4.0, 4.0)
    column_scale = 4.0 ** position * jax.random.uniform(key_cols, (D,), jnp.float32, 0.6, 1.2)
    values = drawn * column_scale
    return values.astype(jnp.bfloat16)


def draw_max_state(key, part):
    key_base = jax.random.fold_in(key, 0)
    drawn = jax.random.uniform(key_base, (SEQS, HEADS), jnp.float32, -3.0, 3.0)
    return drawn


def shard_levels(key, dims, shards, least, high):
    gain, own = 1.0, jax.random.fold_in(key, 6)
    for dim, blocks in shards:
        steps = jnp.exp(jax.random.uniform(jax.random.fold_in(own, dim), (blocks,), jnp.float32, least / len(shards), high / len(shards)))
        gain = gain * jnp.repeat(steps, dims[dim] // blocks).reshape([-1 if axis == dim else 1 for axis in range(len(dims))])
    return gain


def shared_out(own_key, own, number, rows, count, top, limit, skew):
    ranking = jax.random.permutation(own_key, count)
    crowded, ordinary = portions_of(count, rows * top, limit, skew, True), portions_of(count, rows * top, limit, skew, False)
    places = jnp.arange(count)

    def named(lengths, turn):
        used = int((lengths > 0).sum())
        fixed = max(1, used // 4)
        moved = fixed + (places - fixed + turn * (used - fixed)) % max(1, count - fixed)
        return jnp.zeros((count,), jnp.int32).at[ranking[jnp.where(places < fixed, places, moved)]].set(jnp.asarray(lengths, jnp.int32))

    lengths = jnp.where(number % 4 == 0, named(crowded, number // 4), named(ordinary, number - number // 4 - 1))
    mixed = jax.random.permutation(jax.random.fold_in(own, 3), count)
    donor, taker = mixed[0:count // 2 * 2:2], mixed[1:count // 2 * 2:2]
    margin = jnp.minimum(lengths[donor] - 1, limit - lengths[taker]) // 2
    margin = jnp.where((donor == ranking[0]) | (taker == ranking[0]) | (lengths[taker] == 0), 0, jnp.maximum(margin, 0))
    moved = jax.random.randint(jax.random.fold_in(own, 4), (count // 2,), 0, 1 << 20) % (margin + 1)
    lengths = lengths.at[donor].add(-moved).at[taker].add(moved)
    labels = jnp.searchsorted(jnp.cumsum(lengths), jnp.arange(rows * top), side="right").astype(jnp.int32)
    listing = labels.reshape(top, rows).T
    listing = listing[jax.random.permutation(jax.random.fold_in(own, 1), rows)]
    turn = jax.random.randint(jax.random.fold_in(own, 2), (rows, 1), 0, top)
    return jnp.take_along_axis(listing, (jnp.arange(top)[None, :] + turn) % top, axis=1)


def portions_of(number_of, total, limit, skew, full):
    loads = [(1 << 20) // math.isqrt(rank ** skew) + 1 for rank in range(1, number_of + 1)]
    largest = limit if full else min(limit, max(-(-total // number_of), total * loads[0] // sum(loads)))
    least = 1 if total - largest >= number_of - 1 else 0
    given, spare = [largest] + [least] * (number_of - 1), total - largest - least * (number_of - 1)
    while spare > 0:
        free = [i for i in range(1, number_of) if given[i] < largest] or [i for i in range(1, number_of) if given[i] < limit]
        whole, left = sum([loads[i] for i in free]), spare
        for i in free:
            extra = min(limit - given[i], max(1, left * loads[i] // whole), spare)
            given[i] = given[i] + extra
            spare = spare - extra
    return np.array(given)


def bell_draw(rng, shape, scale, reach, pieces=(), held_as=jnp.bfloat16):
    array = scale * jax.random.normal(rng, shape, jnp.float32)
    if pieces:
        array = array * shard_levels(rng, shape, pieces, -0.22, 0.18)
    return jnp.clip(array, -reach, reach).astype(held_as)


def setup_inputs(seed: int = 0, part: int = 0) -> dict:
    keys = jax.random.split(jax.random.key(seed), 22)
    part_splits = jax.random.split(jax.random.fold_in(keys[21], part), 22)
    tokens = draw_tokens(jax.random.fold_in(jax.random.fold_in(keys[21], part), 71), part)
    first_gain = jnp.clip(1.0 + 0.18 * jax.random.normal(keys[1], (D,), jnp.float32), 0.1, 1.9)
    w_query = bell_draw(keys[2], (D, HEADS * DK), D ** -0.5, 0.125, ((0, 16), (1, 16)))
    w_key = bell_draw(keys[3], (D, HEADS * DK), D ** -0.5, 0.125, ((0, 16), (1, 16)))
    w_value = bell_draw(keys[4], (D, HEADS * DV), D ** -0.5, 0.125, ((0, 16), (1, 16)))
    w_outgate = bell_draw(keys[5], (D, HEADS * DV), D ** -0.5, 0.125, ((0, 16), (1, 16)))
    w_input = bell_draw(keys[6], (D, HEADS), D ** -0.5, 0.125)
    w_forget = bell_draw(keys[7], (D, HEADS), D ** -0.5, 0.125)
    input_bias = jnp.clip(jax.random.uniform(keys[8], (HEADS,), jnp.float32, -3.0, 3.0), -3.0, 3.0)
    forget_bias = jnp.clip(jax.random.uniform(keys[9], (HEADS,), jnp.float32, -2.0, 5.0), -2.0, 5.0)
    head_gain = jnp.clip(1.0 + 0.18 * jax.random.normal(keys[10], (HEADS * DV,), jnp.float32), 0.1, 1.9)
    w_project = bell_draw(keys[11], (HEADS * DV, D), (HEADS * DV) ** -0.5, 0.09375, ((0, 16), (1, 16)))
    cell_state = bell_draw(part_splits[12], (SEQS, HEADS, DK, DV), 1.0, 6.0, ((0, 16), (1, 16)), jnp.float32)
    norm_state = bell_draw(part_splits[13], (SEQS, HEADS, DK), 1.0, 6.0, ((0, 16), (1, 16)), jnp.float32)
    max_state = draw_max_state(jax.random.fold_in(jax.random.fold_in(keys[21], part), 71), part)
    second_gain = jnp.clip(1.0 + 0.18 * jax.random.normal(keys[15], (D,), jnp.float32), 0.1, 1.9)
    routes_keys = jax.random.split(jax.random.fold_in(part_splits[16], 1), SEQS // SEQ_DEV)
    routes_turns = jax.random.permutation(jax.random.fold_in(part_splits[16], 3), SEQS // SEQ_DEV)
    routes = jax.vmap(lambda own, number: shared_out(jax.random.fold_in(part_splits[16], 2), own, number, SEQ_DEV, EXPERTS, TOP, CAP, 2))(routes_keys, routes_turns).reshape((SEQS, TOP))
    route_weight = jnp.clip(jnp.exp(jax.random.uniform(part_splits[17], (SEQS, TOP), jnp.float32, math.log(0.2), math.log(1.0))), 0.2, 1.0)
    expert_gate = bell_draw(keys[18], (EXPERTS, D, FF), D ** -0.5, 0.125, ((0, 16), (2, 16)))
    expert_up = bell_draw(keys[19], (EXPERTS, D, FF), D ** -0.5, 0.125, ((0, 16), (2, 16)))
    expert_down = bell_draw(keys[20], (EXPERTS, FF, D), FF ** -0.5, 0.09375, ((0, 16), (1, 16)))
    return dict(tokens=tokens, first_gain=first_gain, w_query=w_query, w_key=w_key, w_value=w_value, w_outgate=w_outgate, w_input=w_input, w_forget=w_forget, input_bias=input_bias, forget_bias=forget_bias, head_gain=head_gain, w_project=w_project, cell_state=cell_state, norm_state=norm_state, max_state=max_state, second_gain=second_gain, routes=routes, route_weight=route_weight, expert_gate=expert_gate, expert_up=expert_up, expert_down=expert_down)


NORM_EPS = 1e-05
HEAD_EPS = 1e-06

def layer_norm(stream_rows, gain_cols):
    values = stream_rows.astype(jnp.float32)
    row_mean = lax.optimization_barrier(jnp.mean(values, axis=1, keepdims=True))
    spread = lax.optimization_barrier(jnp.mean(values * values, axis=1, keepdims=True)) - row_mean * row_mean
    return ((values - row_mean) * lax.rsqrt(spread + NORM_EPS) * gain_cols).astype(jnp.bfloat16)

def routing_tables(routes, route_weight, blocks, capacity, experts):
    seq_total = routes.shape[0]
    seq_local = seq_total // blocks
    expert_ids = lax.broadcasted_iota(jnp.int32, (1, 1, experts), 2)
    matches = routes[:, :, None] == expert_ids
    routed = lax.optimization_barrier(jnp.sum(matches.astype(jnp.int32), axis=1))
    combine = lax.optimization_barrier(jnp.sum(jnp.where(matches, route_weight[:, :, None], 0.0), axis=1))
    running = jnp.cumsum(routed.reshape(blocks, seq_local, experts), axis=1).reshape(seq_total, experts) - routed
    block_ids = lax.broadcasted_iota(jnp.int32, (seq_total, experts), 0) // seq_local
    slot_of = block_ids * capacity + running
    slot_ids = lax.broadcasted_iota(jnp.int32, (experts, blocks * capacity, seq_total), 1)
    placed = (slot_of.T[:, None, :] == slot_ids) & (routed.T[:, None, :] > 0)
    return (placed, jnp.where(placed, combine.T[:, None, :], 0.0))

def reference(tokens, first_gain, w_query, w_key, w_value, w_outgate, w_input, w_forget, input_bias, forget_bias, head_gain, w_project, cell_state, norm_state, max_state, second_gain, routes, route_weight, expert_gate, expert_up, expert_down):
    normed = layer_norm(tokens, first_gain)
    queries = jnp.dot(normed, w_query, preferred_element_type=jnp.float32).astype(jnp.bfloat16)
    key_rows = jnp.dot(normed, w_key, preferred_element_type=jnp.float32).astype(jnp.bfloat16)
    value_rows = jnp.dot(normed, w_value, preferred_element_type=jnp.float32).astype(jnp.bfloat16)
    outgate = jnp.dot(normed, w_outgate, preferred_element_type=jnp.float32).astype(jnp.bfloat16)
    input_pre = jnp.dot(normed, w_input, preferred_element_type=jnp.float32) + input_bias
    forget_pre = jnp.dot(normed, w_forget, preferred_element_type=jnp.float32) + forget_bias
    carried = jax.nn.log_sigmoid(forget_pre) + max_state
    new_max = jnp.maximum(carried, input_pre)
    keep_old = jnp.exp(carried - new_max)
    admit_new = jnp.exp(input_pre - new_max)
    key_float = key_rows.astype(jnp.float32).reshape(SEQS, HEADS, DK)
    value_float = value_rows.astype(jnp.float32).reshape(SEQS, HEADS, DV)
    new_cell = keep_old[:, :, None, None] * cell_state + admit_new[:, :, None, None] * key_float[:, :, :, None] * value_float[:, :, None, :]
    new_norm = keep_old[:, :, None] * norm_state + admit_new[:, :, None] * key_float
    query_float = queries.astype(jnp.float32).reshape(SEQS, HEADS, DK) * DK ** (-0.5)
    readout = jnp.einsum('shk,shkv->shv', query_float, new_cell, precision=lax.Precision.HIGHEST)
    head_mean = lax.optimization_barrier(jnp.mean(readout, axis=2, keepdims=True))
    centred = readout - head_mean
    head_var = lax.optimization_barrier(jnp.mean(centred * centred, axis=2, keepdims=True))
    mixed_heads = ((centred * lax.rsqrt(head_var + HEAD_EPS)).reshape(SEQS, HEADS * DV) * head_gain * jax.nn.sigmoid(outgate.astype(jnp.float32))).astype(jnp.bfloat16)
    mixer_out = jnp.dot(mixed_heads, w_project, preferred_element_type=jnp.float32)
    stream = (tokens.astype(jnp.float32) + mixer_out).astype(jnp.bfloat16)
    second_normed = layer_norm(stream, second_gain)
    placed, weighted = routing_tables(routes, route_weight, N_EP, CAP, EXPERTS)
    picker = placed.astype(jnp.bfloat16)

    def one_expert(running_sum, packed):
        pick_rows, weight_rows, gate_w, up_w, down_w = packed
        chosen = jnp.dot(pick_rows, second_normed, preferred_element_type=jnp.float32).astype(jnp.bfloat16)
        gate_sum = jnp.dot(chosen, gate_w, preferred_element_type=jnp.float32)
        up_sum = jnp.dot(chosen, up_w, preferred_element_type=jnp.float32)
        active = (jax.nn.silu(gate_sum) * up_sum).astype(jnp.bfloat16)
        result = jnp.dot(active, down_w, preferred_element_type=jnp.float32).astype(jnp.bfloat16)
        added = jnp.dot(weight_rows.T, result.astype(jnp.float32), precision=lax.Precision.HIGHEST)
        return (running_sum + added, None)
    moe_out, unused = lax.scan(one_expert, jnp.zeros((SEQS, D), jnp.float32), (picker, weighted, expert_gate, expert_up, expert_down))
    layer_out = (stream.astype(jnp.float32) + moe_out).astype(jnp.bfloat16)
    return (layer_out, new_cell, new_norm, new_max)
```

```python
import functools

import jax
import jax.numpy as jnp
from jax import lax
from jax.experimental import pallas as pl
from jax.experimental.pallas import tpu as pltpu
from jax.sharding import PartitionSpec as P

NORM_EPS = 1e-05
HEAD_EPS = 1e-06
F32 = jnp.float32
BF16 = jnp.bfloat16
LANES = 128
SUB = 8


def iota(shape, dim):
    return lax.broadcasted_iota(jnp.int32, shape, dim)


def total(x):
    return jnp.sum(jnp.sum(x, axis=1, keepdims=True), axis=0, keepdims=True)


def far_first(n):
    order = [n // 2]
    for d in range(1, n // 2):
        order += [n // 2 + d, n // 2 - d]
    if n % 2 == 0:
        return [d for d in order if 0 < d < n]
    return list(range(1, n))


def kernel(
    n_ep, n_tp, seq_local, key_size, value_size,
    tokens_h, gain1_h, wq_h, wk_h, wv_h, wo_h, win_h, wfg_h, ib_h, fb_h, hg_h, wp_h,
    cell_h, norm_h, max_h, gain2_h, routes_h, rw_h, eg_h, eu_h, ed_h,
    out_ref, ncell_ref, nnorm_ref, nmax_ref,
    tokens_v, gain1_v, wq_v, wk_v, wv_v, wo_v, win_v, wfg_v, ib_v, fb_v, hg_v, wp_v,
    cell_v, norm_v, max_v, gain2_v, routes_v, rw_v, eg_v, eu_v, ed_v,
    msg0, rec0, msgv, recv, msg1, rec1, msg2, rec2, msg3, rec3, msg4, rec4, msg5, rec5, msg6, rec6, msg7, rec7, msg8, rec8,
    t8_s, part_s, sum_s, slot_s, wide_s,
    load_sem, send_sem, recv_sem,
):
    ep = lax.axis_index("ep")
    tp = lax.axis_index("tp")
    barrier = pltpu.get_barrier_semaphore()
    ep_peers = [lax.rem(ep + d, n_ep) for d in far_first(n_ep)]
    tp_peers = [lax.rem(tp + d, n_tp) for d in far_first(n_tp)]
    for peer in ep_peers:
        pl.semaphore_signal(barrier, inc=1, device_id={"ep": peer}, device_id_type=pl.DeviceIdType.MESH)
    for peer in tp_peers:
        pl.semaphore_signal(barrier, inc=1, device_id={"tp": peer}, device_id_type=pl.DeviceIdType.MESH)

    sources = (
        tokens_h, gain1_h, wq_h, wk_h, wv_h, wo_h, win_h, wfg_h, ib_h, fb_h, hg_h, wp_h,
        cell_h, norm_h, max_h, gain2_h, routes_h, rw_h, eg_h, eu_h, ed_h,
    )
    targets = (
        tokens_v, gain1_v, wq_v, wk_v, wv_v, wo_v, win_v, wfg_v, ib_v, fb_v, hg_v, wp_v,
        cell_v, norm_v, max_v, gain2_v, routes_v, rw_v, eg_v, eu_v, ed_v,
    )
    loads = [
        pltpu.make_async_copy(s, t, load_sem.at[i]) for i, (s, t) in enumerate(zip(sources, targets))
    ]
    for copy in loads:
        copy.start()

    def send(phase, axis, peers, source, target, each):
        me = ep if axis == "ep" else tp
        for peer in peers:
            pltpu.make_async_remote_copy(
                src_ref=source.at[peer] if each else source,
                dst_ref=target.at[me],
                send_sem=send_sem.at[phase],
                recv_sem=recv_sem.at[phase],
                device_id={axis: peer},
                device_id_type=pl.DeviceIdType.MESH,
            ).start()

    def arrive(phase, target):
        others = target.at[pl.ds(0, target.shape[0] - 1)]
        pltpu.make_async_copy(others, others, recv_sem.at[phase]).wait()

    def drain(phase, target):
        others = target.at[pl.ds(0, target.shape[0] - 1)]
        pltpu.make_async_copy(others, others, send_sem.at[phase]).wait()

    rows8 = max(SUB * n_ep, LANES)
    seqs = n_ep * seq_local
    features = n_ep * LANES
    nt = (((1,), (1,)), ((), ()))
    sub = iota((SUB, LANES), 0)
    lane = iota((SUB, LANES), 1)
    kt = key_size // LANES
    vt = value_size // LANES

    for copy in loads[:6]:
        copy.wait()
    r8 = iota((rows8, seqs), 0)
    pick = ((r8 // SUB) * seq_local + r8 % SUB == iota((rows8, seqs), 1)) & (r8 % SUB < seq_local)
    t8 = jnp.dot(pick.astype(BF16), tokens_v[...], preferred_element_type=F32)
    t8_s[...] = t8
    wide_lane = iota((rows8, LANES), 1)
    row_sum = jnp.sum(t8, axis=1, keepdims=True)
    row_square = jnp.sum(t8 * t8, axis=1, keepdims=True)
    stats = jnp.where(wide_lane == 0, row_sum, jnp.where(wide_lane == 1, row_square, 0.0)).T
    msg0[...] = stats[0:2]
    gain_here = gain1_v[pl.ds(ep, 1), :]
    gain_high = gain_here.astype(BF16).astype(F32)
    kind = iota((rows8, LANES), 0) % SUB
    centred = (t8 - row_sum * (1.0 / LANES)) * gain_here
    left = jnp.where(
        kind == seq_local, gain_high, jnp.where(kind == seq_local + 1, gain_here - gain_high, centred)
    ).astype(BF16)
    at = 0
    for w in (wv_v, wo_v):
        part = jnp.dot(left, w[...], preferred_element_type=F32)
        for j in range(vt):
            part_s[at] = part[:, j * LANES:(j + 1) * LANES]
            at += 1
    for j in range(2 * vt):
        gain_term = part_s[j, pl.ds(seq_local, 1), :] + part_s[j, pl.ds(seq_local + 1, 1), :]
        term_high = gain_term.astype(BF16).astype(F32)
        part_s[j, pl.ds(seq_local, n_ep, SUB), :] = jnp.broadcast_to(term_high, (n_ep, LANES))
        part_s[j, pl.ds(seq_local + 1, n_ep, SUB), :] = jnp.broadcast_to(
            gain_term - term_high, (n_ep, LANES)
        )
    for p in range(n_ep):
        rows = slice(p * SUB, (p + 1) * SUB)
        for j in range(vt):
            msgv[p, :, j * LANES:(j + 1) * LANES] = jnp.concatenate(
                [part_s[j, rows, :], part_s[vt + j, rows, :]], axis=0
            ).astype(BF16)

    pl.semaphore_wait(barrier, len(ep_peers) + len(tp_peers))
    send(0, "ep", ep_peers, msg0, rec0, False)
    send(9, "ep", ep_peers, msgv, recv, True)
    rec0[ep] = msg0[...]
    recv[ep] = msgv[ep]

    for copy in loads[6:18]:
        copy.wait()
    here = pl.ds(pl.multiple_of(ep * LANES, LANES), LANES)
    gate_w = jnp.zeros((SUB, LANES), F32)
    for row, source in enumerate((win_v, wfg_v)):
        head = (iota((SUB, n_tp), 1) == tp) & (iota((SUB, n_tp), 0) == row)
        gate_w = gate_w + jnp.dot(head.astype(BF16), source[:, here], preferred_element_type=F32)
    gate_w = gate_w.astype(BF16)
    at_head = iota((1, n_tp), 1) == tp
    input_bias = jnp.sum(jnp.where(at_head, ib_v[...], 0.0), axis=1, keepdims=True)
    forget_bias = jnp.sum(jnp.where(at_head, fb_v[...], 0.0), axis=1, keepdims=True)

    top = routes_v.shape[0]
    own_row = iota((SUB, seqs), 1) == tp * seq_local + iota((SUB, seqs), 0)
    own_row = own_row & (iota((SUB, seqs), 0) < seq_local)
    routed = jnp.zeros((SUB, LANES), F32)
    combine = jnp.zeros((SUB, LANES), F32)
    for k in range(top):
        named = jnp.sum(
            jnp.where(own_row, routes_v[k:k + 1, :].astype(F32) + 1.0, 0.0), axis=1, keepdims=True
        )
        weight = jnp.sum(jnp.where(own_row, rw_v[k:k + 1, :], 0.0), axis=1, keepdims=True)
        match = jnp.abs(named - 1.0 - (lane // SUB).astype(F32)) < 0.5
        routed = routed + jnp.where(match, 1.0, 0.0)
        combine = combine + jnp.where(match, weight, 0.0)
    before = (iota((SUB, SUB), 1) < iota((SUB, SUB), 0)).astype(BF16)
    running = jnp.dot(before, routed.astype(BF16), preferred_element_type=F32)
    placed = jnp.where((routed > 0.5) & (jnp.abs(running - (lane % SUB).astype(F32)) < 0.5), 1.0, 0.0)
    slot_weight = placed * combine
    weight_high = slot_weight.astype(BF16)
    rest = slot_weight - weight_high.astype(F32)
    weight_mid = rest.astype(BF16)
    weight_low = (rest - weight_mid.astype(F32)).astype(BF16)
    capacity = 2
    chosen = [
        jnp.sum(jnp.where(lane == ep * SUB + c, placed, 0.0), axis=1, keepdims=True) for c in range(capacity)
    ]

    arrive(0, rec0)
    stat = rec0[0]
    for e in range(n_ep):
        if e:
            stat = stat + rec0[e]
        sum_s[e:e + 1, :] = rec0[e, 0:1, :]
    stat8 = jnp.where(sub == 0, stat[0:1], jnp.where(sub == 1, stat[1:2], 0.0))
    column = stat8.T
    mean = column[:, 0:1] * (1.0 / features)
    spread = column[:, 1:2] * (1.0 / features) - mean * mean
    normed = ((t8_s[...] - mean) * lax.rsqrt(spread + NORM_EPS) * gain_here).astype(BF16)
    gate_rows = lax.dot_general(gate_w, normed, nt, preferred_element_type=F32)
    for j, w in enumerate((wq_v, wk_v)):
        part = jnp.dot(normed, w[...], preferred_element_type=F32)
        part = jnp.where(kind == seq_local, gate_rows[j:j + 1], part)
        for p in range(n_ep):
            msg1[p, :, j * LANES:(j + 1) * LANES] = part[p * SUB:(p + 1) * SUB]
    send(1, "ep", ep_peers, msg1, rec1, True)
    rec1[ep] = msg1[ep]

    mine = (lane == ep * SUB + sub) & (sub < seq_local)
    own_mean = jnp.sum(jnp.where(mine, stat[0:1], 0.0), axis=1, keepdims=True) * (1.0 / features)
    own_square = jnp.sum(jnp.where(mine, stat[1:2], 0.0), axis=1, keepdims=True) * (1.0 / features)
    own_inv = lax.rsqrt(own_square - own_mean * own_mean + NORM_EPS)
    off = lax.dot_general(
        jnp.where(mine, 1.0, 0.0), sum_s[...], nt,
        preferred_element_type=F32, precision=lax.Precision.HIGHEST,
    ) * (1.0 / LANES) - own_mean
    arrive(9, recv)
    for e in range(n_ep):
        arrived = recv[e].astype(F32)
        for j in range(vt):
            piece = arrived[:, j * LANES:(j + 1) * LANES]
            part_s[j, e * SUB:(e + 1) * SUB, :] = piece[:SUB]
            part_s[vt + j, e * SUB:(e + 1) * SUB, :] = piece[SUB:]
    rest_of = []
    for j in range(2 * vt):
        acc = part_s[j, 0:SUB, :]
        for e in range(1, n_ep):
            acc = acc + part_s[j, e * SUB:(e + 1) * SUB, :]
        gain_terms = part_s[j, pl.ds(seq_local, n_ep, SUB), :] + part_s[j, pl.ds(seq_local + 1, n_ep, SUB), :]
        acc = acc + jnp.dot(
            off, gain_terms, preferred_element_type=F32, precision=lax.Precision.HIGHEST
        )
        rest_of.append(jnp.where(sub < seq_local, acc * own_inv, 0.0).astype(BF16).astype(F32))
    value = jnp.concatenate(rest_of[:vt], axis=1)
    outgate = jax.nn.sigmoid(jnp.concatenate(rest_of[vt:], axis=1))
    max8 = jnp.zeros((SUB, LANES), F32)
    for i in range(seq_local):
        max8 = jnp.where(sub == i, max_v[:, i:i + 1], max8)
    head_gain = jnp.concatenate([hg_v[pl.ds(tp * vt + j, 1), :] for j in range(vt)], axis=1)
    wide_p = jnp.concatenate([wp_v[j * LANES:(j + 1) * LANES, :] for j in range(vt)], axis=1)

    arrive(1, rec1)
    sums = rec1[0]
    for e in range(1, n_ep):
        sums = sums + rec1[e]
    in8 = jnp.sum(
        jnp.where(mine, sums[seq_local:seq_local + 1, :LANES], 0.0), axis=1, keepdims=True
    ) + input_bias
    fg8 = jnp.sum(
        jnp.where(mine, sums[seq_local:seq_local + 1, LANES:2 * LANES], 0.0), axis=1, keepdims=True
    ) + forget_bias
    carried = jnp.minimum(fg8, 0.0) - jnp.log1p(jnp.exp(-jnp.abs(fg8))) + max8
    new_max = jnp.maximum(carried, in8)
    keep = jnp.exp(carried - new_max)
    admit = jnp.exp(in8 - new_max)
    across = jnp.sum(jnp.where(sub == iota((SUB, LANES), 1), new_max, 0.0), axis=0, keepdims=True)
    nmax_ref[...] = across[:, :seq_local]
    query = sums[:, :LANES].astype(BF16).astype(F32) * key_size ** (-0.5)
    admitted = admit * sums[:, LANES:2 * LANES].astype(BF16).astype(F32)
    query_t = query.T
    admitted_t = admitted.T
    sub_wide = iota((SUB, value_size), 0)
    readout = jnp.zeros((SUB, value_size), F32)
    for i in range(seq_local):
        nnorm_ref[i] = keep[i:i + 1] * norm_v[i] + admitted[i:i + 1]
        new_cell = keep[i:i + 1, 0:1] * cell_v[i, 0] + admitted_t[:, i:i + 1] * value[i:i + 1, :]
        ncell_ref[i, 0] = new_cell
        read = jnp.sum(query_t[:, i:i + 1] * new_cell, axis=0, keepdims=True)
        readout = jnp.where(sub_wide == i, read, readout)
    head_mean = jnp.mean(readout, axis=1, keepdims=True)
    spread_out = readout - head_mean
    head_var = jnp.mean(spread_out * spread_out, axis=1, keepdims=True)
    mixed = spread_out * lax.rsqrt(head_var + HEAD_EPS) * head_gain * outgate
    mixed = jnp.concatenate([mixed[:, j * LANES:(j + 1) * LANES] for j in range(vt)], axis=0).astype(BF16)
    msg2[...] = mixed

    send(2, "ep", ep_peers, msg2, rec2, False)
    rec2[ep] = mixed
    arrive(2, rec2)
    terms = jnp.dot(
        rec2[...].reshape(n_ep * vt * SUB, LANES), wide_p, preferred_element_type=F32
    )
    for p in range(n_ep):
        term = jnp.zeros((SUB, LANES), F32)
        for j in range(vt):
            start = (p * vt + j) * SUB
            term = term + terms[start:start + SUB, j * LANES:(j + 1) * LANES]
        msg3[p] = term
    send(3, "tp", tp_peers, msg3, rec3, True)
    rec3[tp] = msg3[tp]
    arrive(3, rec3)
    mixer = rec3[0]
    for t in range(1, n_tp):
        mixer = mixer + rec3[t]
    stream16 = (t8_s[pl.ds(pl.multiple_of(tp * SUB, SUB), SUB), :] + mixer).astype(BF16)
    stream = stream16.astype(F32)
    msg4[...] = stream16

    send(4, "ep", ep_peers, msg4, rec4, False)
    rec4[ep] = stream16
    gain2 = gain2_v[...]
    arrive(4, rec4)
    for e in range(n_ep):
        slot_s[e * SUB:(e + 1) * SUB, :] = rec4[e].astype(F32)
    rows_of = [slot_s[pl.ds(r, n_ep, SUB), :] for r in range(seq_local)]
    slots = []
    for c in range(capacity):
        x = chosen[c][0:1, :] * rows_of[0]
        for r in range(1, seq_local):
            x = x + chosen[c][r:r + 1, :] * rows_of[r]
        mean = total(x) * (1.0 / features)
        spread = total(x * x) * (1.0 / features) - mean * mean
        slots.append((x - mean) * lax.rsqrt(spread + NORM_EPS) * gain2)
    slots16 = jnp.concatenate(slots, axis=0).astype(BF16)
    msg5[...] = slots16

    send(5, "tp", tp_peers, msg5, rec5, False)
    rec5[tp] = slots16
    for copy in loads[18:]:
        copy.wait()
    arrive(5, rec5)
    rows_c = capacity * n_ep
    slot_count = capacity * n_tp
    for t in range(n_tp):
        wide_s[t * rows_c:(t + 1) * rows_c, :] = rec5[t].astype(F32)
    x = jnp.concatenate(
        [wide_s[pl.ds(e, slot_count, n_ep), :].astype(BF16) for e in range(n_ep)], axis=1
    )
    gate = jnp.dot(x, eg_v[0], preferred_element_type=F32)
    up = jnp.dot(x, eu_v[0], preferred_element_type=F32)
    active = (jax.nn.silu(gate) * up).astype(BF16)
    down = jnp.dot(active, ed_v[0], preferred_element_type=F32)
    for e in range(n_ep):
        wide_s[pl.ds(e, slot_count, n_ep), :] = down[:, e * LANES:(e + 1) * LANES]
    for t in range(n_tp):
        msg6[t] = wide_s[t * rows_c:(t + 1) * rows_c, :].astype(BF16)
    send(6, "tp", tp_peers, msg6, rec6, True)
    rec6[tp] = msg6[tp]
    slot_s[...] = jnp.zeros_like(slot_s)
    arrive(6, rec6)
    done = rec6[0].astype(F32)
    for t in range(1, n_tp):
        done = done + rec6[t].astype(F32)
    for c in range(capacity):
        slot_s[pl.ds(c, n_ep, SUB), :] = done[c * n_ep:(c + 1) * n_ep]
    for e in range(n_ep):
        msg7[e] = slot_s[e * SUB:(e + 1) * SUB, :].astype(BF16)

    send(7, "ep", ep_peers, msg7, rec7, True)
    rec7[ep] = msg7[ep]
    arrive(7, rec7)
    returned = jnp.concatenate([rec7[e].astype(F32) for e in range(n_ep)], axis=0).astype(BF16)
    lhs = jnp.concatenate(
        [weight_high.astype(F32), weight_mid.astype(F32), weight_low.astype(F32)], axis=0
    )[:, :SUB * n_ep].astype(BF16)
    moe = jnp.dot(lhs, returned, preferred_element_type=F32)
    moe = moe[0:SUB] + moe[SUB:2 * SUB] + moe[2 * SUB:3 * SUB]
    layer16 = (stream + moe).astype(BF16)
    msg8[...] = layer16
    send(8, "tp", tp_peers, msg8, rec8, False)
    rec8[tp] = layer16
    arrive(8, rec8)
    finished = jnp.concatenate([rec8[t].astype(F32) for t in range(n_tp)], axis=0).astype(BF16)
    c8 = iota((seqs, SUB * n_tp), 1)
    unpick = (c8 // SUB) * seq_local + c8 % SUB == iota((seqs, SUB * n_tp), 0)
    unpick = unpick & (c8 % SUB < seq_local)
    out_ref[...] = jnp.dot(unpick.astype(BF16), finished, preferred_element_type=F32).astype(BF16)

    for phase, target in enumerate((rec0, rec1, rec2, rec3, rec4, rec5, rec6, rec7, rec8, recv)):
        drain(phase, target)


def solution(mesh):
    n_ep = mesh.shape["ep"]
    n_tp = mesh.shape["tp"]

    def on_device(*args):
        (
            tokens, first_gain, w_query, w_key, w_value, w_outgate, w_input, w_forget,
            input_bias, forget_bias, head_gain, w_project, cell_state, norm_state, max_state,
            second_gain, routes, route_weight, expert_gate, expert_up, expert_down,
        ) = args
        seq_local = tokens.shape[0] // n_ep
        key_size, value_size = cell_state.shape[2], cell_state.shape[3]
        capacity = 2
        operands = (
            tokens, first_gain.reshape(n_ep, LANES), w_query, w_key, w_value, w_outgate,
            w_input.T, w_forget.T, input_bias.reshape(1, -1), forget_bias.reshape(1, -1),
            head_gain.reshape(-1, LANES), w_project, cell_state, norm_state, max_state.T,
            second_gain.reshape(n_ep, LANES), routes.T, route_weight.T,
            expert_gate, expert_up, expert_down,
        )
        hbm = pl.BlockSpec(memory_space=pltpu.HBM)
        vmem = pl.BlockSpec(memory_space=pltpu.VMEM)
        rows8 = max(SUB * n_ep, LANES)
        vt = value_size // LANES

        def pair(shape_out, shape_in, dtype):
            return [pltpu.VMEM(shape_out, dtype), pltpu.VMEM(shape_in, dtype)]

        messages = (
            pair((2, rows8), (n_ep, 2, rows8), F32)
            + pair((n_ep, 2 * SUB, value_size), (n_ep, 2 * SUB, value_size), BF16)
            + pair((n_ep, SUB, 2 * key_size), (n_ep, SUB, 2 * key_size), F32)
            + pair((vt * SUB, LANES), (n_ep, vt * SUB, LANES), BF16)
            + pair((n_tp, SUB, LANES), (n_tp, SUB, LANES), F32)
            + pair((SUB, LANES), (n_ep, SUB, LANES), BF16)
            + pair((capacity * n_ep, LANES), (n_tp, capacity * n_ep, LANES), BF16)
            + pair((n_tp, capacity * n_ep, LANES), (n_tp, capacity * n_ep, LANES), BF16)
            + pair((n_ep, SUB, LANES), (n_ep, SUB, LANES), BF16)
            + pair((SUB, LANES), (n_tp, SUB, LANES), BF16)
        )
        out, new_cell, new_norm, new_max = pl.pallas_call(
            functools.partial(kernel, n_ep, n_tp, seq_local, key_size, value_size),
            out_shape=(
                jax.ShapeDtypeStruct(tokens.shape, BF16),
                jax.ShapeDtypeStruct(cell_state.shape, F32),
                jax.ShapeDtypeStruct(norm_state.shape, F32),
                jax.ShapeDtypeStruct((1, seq_local), F32),
            ),
            in_specs=[hbm] * len(operands),
            out_specs=(vmem, vmem, vmem, vmem),
            scratch_shapes=[pltpu.VMEM(a.shape, a.dtype) for a in operands]
            + messages
            + [
                pltpu.VMEM((rows8, LANES), F32),
                pltpu.VMEM((2 * vt, rows8, LANES), F32),
                pltpu.VMEM((n_ep, rows8), F32),
                pltpu.VMEM((SUB * n_ep, LANES), F32),
                pltpu.VMEM((n_tp * capacity * n_ep, LANES), F32),
                pltpu.SemaphoreType.DMA((len(operands),)),
                pltpu.SemaphoreType.DMA((10,)),
                pltpu.SemaphoreType.DMA((10,)),
            ],
            compiler_params=pltpu.CompilerParams(
                collective_id=0, has_side_effects=True
            ),
        )(*operands)
        return out, new_cell, new_norm, new_max.T

    placed = (
        P("grp", "ep"), P(), P("ep", "tp"), P("ep", "tp"), P("ep", "tp"), P("ep", "tp"),
        P(), P(), P(), P(), P(), P("tp", "ep"),
        P(("grp", "ep"), "tp", None, None), P(("grp", "ep"), "tp", None), P(("grp", "ep"), "tp"),
        P(), P("grp", None), P("grp", None),
        P("ep", None, "tp"), P("ep", None, "tp"), P("ep", "tp", None),
    )
    return jax.shard_map(
        on_device,
        mesh=mesh,
        in_specs=placed,
        out_specs=(
            P("grp", "ep"),
            P(("grp", "ep"), "tp", None, None),
            P(("grp", "ep"), "tp", None),
            P(("grp", "ep"), "tp"),
        ),
        check_vma=False,
    )
```

```python
import functools

import jax
import jax.numpy as jnp
from jax import lax
from jax.experimental import pallas as pl
from jax.experimental.pallas import tpu as pltpu
from jax.sharding import PartitionSpec as P

NORM_EPS = 1e-05
HEAD_EPS = 1e-06
F32 = jnp.float32
BF16 = jnp.bfloat16
LANES = 128
SUB = 8


def iota(shape, dim):
    return lax.broadcasted_iota(jnp.int32, shape, dim)


def total(x):
    return jnp.sum(jnp.sum(x, axis=1, keepdims=True), axis=0, keepdims=True)


def far_first(n):
    order = [n // 2]
    for d in range(1, n // 2):
        order += [n // 2 + d, n // 2 - d]
    if n % 2 == 0:
        return [d for d in order if 0 < d < n]
    return list(range(1, n))


def kernel(
    n_ep, n_tp, seq_local, key_size, value_size,
    tokens_h, gain1_h, wq_h, wk_h, wv_h, wo_h, win_h, wfg_h, ib_h, fb_h, hg_h, wp_h,
    cell_h, norm_h, max_h, gain2_h, routes_h, rw_h, eg_h, eu_h, ed_h,
    out_ref, ncell_ref, nnorm_ref, nmax_ref,
    tokens_v, gain1_v, wq_v, wk_v, wv_v, wo_v, win_v, wfg_v, ib_v, fb_v, hg_v, wp_v,
    cell_v, norm_v, max_v, gain2_v, routes_v, rw_v, eg_v, eu_v, ed_v,
    msg0, rec0, msgv, recv, msg1, rec1, msg2, rec2, msg3, rec3, msg4, rec4, msg5, rec5, msg6, rec6, msg7, rec7, msg8, rec8,
    t8_s, part_s, sum_s, slot_s, wide_s,
    load_sem, send_sem, recv_sem, known_sem,
):
    ep = lax.axis_index("ep")
    tp = lax.axis_index("tp")
    barrier = pltpu.get_barrier_semaphore()
    rec7[...] = jnp.zeros_like(rec7)
    rec8[...] = jnp.zeros_like(rec8)
    ep_peers = [lax.rem(ep + d, n_ep) for d in far_first(n_ep)]
    tp_peers = [lax.rem(tp + d, n_tp) for d in far_first(n_tp)]
    for peer in ep_peers:
        pl.semaphore_signal(barrier, inc=1, device_id={"ep": peer}, device_id_type=pl.DeviceIdType.MESH)

    def tell(sem, reach):
        for d in (reach, n_tp - reach):
            peer = lax.rem(tp + d, n_tp)
            pl.semaphore_signal(sem, inc=1, device_id={"tp": peer}, device_id_type=pl.DeviceIdType.MESH)

    tell(barrier, 1)

    sources = (
        tokens_h, gain1_h, wq_h, wk_h, wv_h, wo_h, win_h, wfg_h, ib_h, fb_h, hg_h, wp_h,
        cell_h, norm_h, max_h, gain2_h, routes_h, rw_h, eg_h, eu_h, ed_h,
    )
    targets = (
        tokens_v, gain1_v, wq_v, wk_v, wv_v, wo_v, win_v, wfg_v, ib_v, fb_v, hg_v, wp_v,
        cell_v, norm_v, max_v, gain2_v, routes_v, rw_v, eg_v, eu_v, ed_v,
    )
    loads = [
        pltpu.make_async_copy(s, t, load_sem.at[i]) for i, (s, t) in enumerate(zip(sources, targets))
    ]
    for copy in loads:
        copy.start()

    def send(phase, axis, peers, source, target, each, used=None):
        me = ep if axis == "ep" else tp
        used = pl.ds(0, target.shape[1] if used is None else used)
        for peer in peers:
            pltpu.make_async_remote_copy(
                src_ref=source.at[peer, used] if each else source.at[used],
                dst_ref=target.at[me, used],
                send_sem=send_sem.at[phase],
                recv_sem=recv_sem.at[phase],
                device_id={axis: peer},
                device_id_type=pl.DeviceIdType.MESH,
            ).start()

    def settle(sem, target, used):
        used = target.shape[1] if used is None else used
        others = target.at[pl.ds(0, target.shape[0] - 1), pl.ds(0, used)]
        pltpu.make_async_copy(others, others, sem).wait()

    def arrive(phase, target, used=None):
        settle(recv_sem.at[phase], target, used)

    rows8 = max(SUB * n_ep, LANES)
    seqs = n_ep * seq_local
    features = n_ep * LANES
    nt = (((1,), (1,)), ((), ()))
    sub = iota((SUB, LANES), 0)
    lane = iota((SUB, LANES), 1)
    kt = key_size // LANES
    vt = value_size // LANES

    for copy in loads[:6]:
        copy.wait()
    r8 = iota((rows8, seqs), 0)
    pick = ((r8 // SUB) * seq_local + r8 % SUB == iota((rows8, seqs), 1)) & (r8 % SUB < seq_local)
    t8 = jnp.dot(pick.astype(BF16), tokens_v[...], preferred_element_type=F32)
    t8_s[...] = t8
    wide_lane = iota((rows8, LANES), 1)
    row_sum = jnp.sum(t8, axis=1, keepdims=True)
    row_square = jnp.sum(t8 * t8, axis=1, keepdims=True)
    stats = jnp.where(wide_lane == 0, row_sum, jnp.where(wide_lane == 1, row_square, 0.0)).T
    msg0[...] = stats[0:2]
    gain_here = gain1_v[pl.ds(ep, 1), :]
    gain_high = gain_here.astype(BF16).astype(F32)
    kind = iota((rows8, LANES), 0) % SUB
    centred = (t8 - row_sum * (1.0 / LANES)) * gain_here
    left = jnp.where(
        kind == seq_local, gain_high, jnp.where(kind == seq_local + 1, gain_here - gain_high, centred)
    ).astype(BF16)
    at = 0
    for w in (wv_v, wo_v):
        part = jnp.dot(left, w[...], preferred_element_type=F32)
        for j in range(vt):
            part_s[at] = part[:, j * LANES:(j + 1) * LANES]
            at += 1
    for j in range(2 * vt):
        gain_term = part_s[j, pl.ds(seq_local, 1), :] + part_s[j, pl.ds(seq_local + 1, 1), :]
        term_high = gain_term.astype(BF16).astype(F32)
        part_s[j, pl.ds(seq_local, n_ep, SUB), :] = jnp.broadcast_to(term_high, (n_ep, LANES))
        part_s[j, pl.ds(seq_local + 1, n_ep, SUB), :] = jnp.broadcast_to(
            gain_term - term_high, (n_ep, LANES)
        )
    for p in range(n_ep):
        rows = slice(p * SUB, (p + 1) * SUB)
        for j in range(vt):
            msgv[p, :, j * LANES:(j + 1) * LANES] = jnp.concatenate(
                [part_s[j, rows, :], part_s[vt + j, rows, :]], axis=0
            ).astype(BF16)

    pl.semaphore_wait(barrier, len(ep_peers) + 2)
    rounds = [1]
    while 2 * rounds[-1] < n_tp // 2:
        rounds.append(2 * rounds[-1])
    send(0, "ep", ep_peers, msg0, rec0, False)
    send(9, "ep", ep_peers, msgv, recv, True)
    rec0[ep] = msg0[...]
    recv[ep] = msgv[ep]

    tell(known_sem.at[0], rounds[0])

    for copy in loads[6:18]:
        copy.wait()
    here = pl.ds(pl.multiple_of(ep * LANES, LANES), LANES)
    gate_w = jnp.zeros((SUB, LANES), F32)
    for row, source in enumerate((win_v, wfg_v)):
        head = (iota((SUB, n_tp), 1) == tp) & (iota((SUB, n_tp), 0) == row)
        gate_w = gate_w + jnp.dot(head.astype(BF16), source[:, here], preferred_element_type=F32)
    gate_w = gate_w.astype(BF16)
    at_head = iota((1, n_tp), 1) == tp
    input_bias = jnp.sum(jnp.where(at_head, ib_v[...], 0.0), axis=1, keepdims=True)
    forget_bias = jnp.sum(jnp.where(at_head, fb_v[...], 0.0), axis=1, keepdims=True)

    top = routes_v.shape[0]
    own_row = iota((SUB, seqs), 1) == tp * seq_local + iota((SUB, seqs), 0)
    own_row = own_row & (iota((SUB, seqs), 0) < seq_local)
    routed = jnp.zeros((SUB, LANES), F32)
    combine = jnp.zeros((SUB, LANES), F32)
    for k in range(top):
        named = jnp.sum(
            jnp.where(own_row, routes_v[k:k + 1, :].astype(F32) + 1.0, 0.0), axis=1, keepdims=True
        )
        weight = jnp.sum(jnp.where(own_row, rw_v[k:k + 1, :], 0.0), axis=1, keepdims=True)
        match = jnp.abs(named - 1.0 - (lane // SUB).astype(F32)) < 0.5
        routed = routed + jnp.where(match, 1.0, 0.0)
        combine = combine + jnp.where(match, weight, 0.0)
    before = (iota((SUB, SUB), 1) < iota((SUB, SUB), 0)).astype(BF16)
    running = jnp.dot(before, routed.astype(BF16), preferred_element_type=F32)
    placed = jnp.where((routed > 0.5) & (jnp.abs(running - (lane % SUB).astype(F32)) < 0.5), 1.0, 0.0)
    slot_weight = placed * combine
    weight_high = slot_weight.astype(BF16)
    rest = slot_weight - weight_high.astype(F32)
    weight_mid = rest.astype(BF16)
    weight_low = (rest - weight_mid.astype(F32)).astype(BF16)
    capacity = 2
    chosen = [
        jnp.sum(jnp.where(lane == ep * SUB + c, placed, 0.0), axis=1, keepdims=True) for c in range(capacity)
    ]

    if len(rounds) > 1:
        pl.semaphore_wait(known_sem.at[0], 2)
        tell(known_sem.at[1], rounds[1])
    arrive(0, rec0)
    stat = rec0[0]
    for e in range(n_ep):
        if e:
            stat = stat + rec0[e]
        sum_s[e:e + 1, :] = rec0[e, 0:1, :]
    stat8 = jnp.where(sub == 0, stat[0:1], jnp.where(sub == 1, stat[1:2], 0.0))
    column = stat8.T
    mean = column[:, 0:1] * (1.0 / features)
    spread = column[:, 1:2] * (1.0 / features) - mean * mean
    normed = ((t8_s[...] - mean) * lax.rsqrt(spread + NORM_EPS) * gain_here).astype(BF16)
    gate_rows = lax.dot_general(gate_w, normed, nt, preferred_element_type=F32)
    for j, w in enumerate((wq_v, wk_v)):
        part = jnp.dot(normed, w[...], preferred_element_type=F32)
        part = jnp.where(kind == seq_local, gate_rows[j:j + 1], part)
        for p in range(n_ep):
            msg1[p, :, j * LANES:(j + 1) * LANES] = part[p * SUB:(p + 1) * SUB]
    q_rows = seq_local + 1
    send(1, "ep", ep_peers, msg1, rec1, True, q_rows)
    rec1[ep] = msg1[ep]

    mine = (lane == ep * SUB + sub) & (sub < seq_local)
    own_mean = jnp.sum(jnp.where(mine, stat[0:1], 0.0), axis=1, keepdims=True) * (1.0 / features)
    own_square = jnp.sum(jnp.where(mine, stat[1:2], 0.0), axis=1, keepdims=True) * (1.0 / features)
    own_inv = lax.rsqrt(own_square - own_mean * own_mean + NORM_EPS)
    off = lax.dot_general(
        jnp.where(mine, 1.0, 0.0), sum_s[...], nt,
        preferred_element_type=F32, precision=lax.Precision.HIGHEST,
    ) * (1.0 / LANES) - own_mean
    if len(rounds) > 2:
        pl.semaphore_wait(known_sem.at[1], 2)
        tell(known_sem.at[2], rounds[2])
    arrive(9, recv)
    for e in range(n_ep):
        arrived = recv[e].astype(F32)
        for j in range(vt):
            piece = arrived[:, j * LANES:(j + 1) * LANES]
            part_s[j, e * SUB:(e + 1) * SUB, :] = piece[:SUB]
            part_s[vt + j, e * SUB:(e + 1) * SUB, :] = piece[SUB:]
    rest_of = []
    for j in range(2 * vt):
        acc = part_s[j, 0:SUB, :]
        for e in range(1, n_ep):
            acc = acc + part_s[j, e * SUB:(e + 1) * SUB, :]
        gain_terms = part_s[j, pl.ds(seq_local, n_ep, SUB), :] + part_s[j, pl.ds(seq_local + 1, n_ep, SUB), :]
        acc = acc + jnp.dot(
            off, gain_terms, preferred_element_type=F32, precision=lax.Precision.HIGHEST
        )
        rest_of.append(jnp.where(sub < seq_local, acc * own_inv, 0.0).astype(BF16).astype(F32))
    value = jnp.concatenate(rest_of[:vt], axis=1)
    outgate = jax.nn.sigmoid(jnp.concatenate(rest_of[vt:], axis=1))
    max8 = jnp.zeros((SUB, LANES), F32)
    for i in range(seq_local):
        max8 = jnp.where(sub == i, max_v[:, i:i + 1], max8)
    head_gain = jnp.concatenate([hg_v[pl.ds(tp * vt + j, 1), :] for j in range(vt)], axis=1)
    wide_p = jnp.concatenate([wp_v[j * LANES:(j + 1) * LANES, :] for j in range(vt)], axis=1)

    arrive(1, rec1, q_rows)
    sums = rec1[0]
    for e in range(1, n_ep):
        sums = sums + rec1[e]
    in8 = jnp.sum(
        jnp.where(mine, sums[seq_local:seq_local + 1, :LANES], 0.0), axis=1, keepdims=True
    ) + input_bias
    fg8 = jnp.sum(
        jnp.where(mine, sums[seq_local:seq_local + 1, LANES:2 * LANES], 0.0), axis=1, keepdims=True
    ) + forget_bias
    carried = jnp.minimum(fg8, 0.0) - jnp.log1p(jnp.exp(-jnp.abs(fg8))) + max8
    new_max = jnp.maximum(carried, in8)
    keep = jnp.exp(carried - new_max)
    admit = jnp.exp(in8 - new_max)
    across = jnp.sum(jnp.where(sub == iota((SUB, LANES), 1), new_max, 0.0), axis=0, keepdims=True)
    nmax_ref[...] = across[:, :seq_local]
    sums = jnp.where(iota((SUB, 2 * LANES), 0) < seq_local, sums, 0.0)
    query = sums[:, :LANES].astype(BF16).astype(F32) * key_size ** (-0.5)
    admitted = admit * sums[:, LANES:2 * LANES].astype(BF16).astype(F32)
    query_t = query.T
    admitted_t = admitted.T
    sub_wide = iota((SUB, value_size), 0)
    readout = jnp.zeros((SUB, value_size), F32)
    for i in range(seq_local):
        nnorm_ref[i] = keep[i:i + 1] * norm_v[i] + admitted[i:i + 1]
        new_cell = keep[i:i + 1, 0:1] * cell_v[i, 0] + admitted_t[:, i:i + 1] * value[i:i + 1, :]
        ncell_ref[i, 0] = new_cell
        read = jnp.sum(query_t[:, i:i + 1] * new_cell, axis=0, keepdims=True)
        readout = jnp.where(sub_wide == i, read, readout)
    head_mean = jnp.mean(readout, axis=1, keepdims=True)
    spread_out = readout - head_mean
    head_var = jnp.mean(spread_out * spread_out, axis=1, keepdims=True)
    mixed = spread_out * lax.rsqrt(head_var + HEAD_EPS) * head_gain * outgate
    mixed = jnp.concatenate([mixed[:, j * LANES:(j + 1) * LANES] for j in range(vt)], axis=0).astype(BF16)
    msg2[...] = mixed

    send(2, "ep", ep_peers, msg2, rec2, False)
    rec2[ep] = mixed
    arrive(2, rec2)
    terms = jnp.dot(
        rec2[...].reshape(n_ep * vt * SUB, LANES), wide_p, preferred_element_type=F32
    )
    for p in range(n_ep):
        term = jnp.zeros((SUB, LANES), F32)
        for j in range(vt):
            start = (p * vt + j) * SUB
            term = term + terms[start:start + SUB, j * LANES:(j + 1) * LANES]
        msg3[p] = term.astype(BF16)
    last = len(rounds) - 1
    pl.semaphore_wait(known_sem.at[last], 2)
    send(3, "tp", tp_peers, msg3, rec3, True, seq_local)
    rec3[tp] = msg3[tp]
    arrive(3, rec3, seq_local)
    mixer = rec3[0].astype(F32)
    for t in range(1, n_tp):
        mixer = mixer + rec3[t].astype(F32)
    mixer = jnp.where(sub < seq_local, mixer, 0.0)
    stream16 = (t8_s[pl.ds(pl.multiple_of(tp * SUB, SUB), SUB), :] + mixer).astype(BF16)
    stream = stream16.astype(F32)
    msg4[...] = stream16

    send(4, "ep", ep_peers, msg4, rec4, False, seq_local)
    rec4[ep] = stream16
    gain2 = gain2_v[...]
    arrive(4, rec4, seq_local)
    for e in range(n_ep):
        slot_s[e * SUB:(e + 1) * SUB, :] = rec4[e].astype(F32)
    rows_of = [slot_s[pl.ds(r, n_ep, SUB), :] for r in range(seq_local)]
    slots = []
    for c in range(capacity):
        x = chosen[c][0:1, :] * rows_of[0]
        for r in range(1, seq_local):
            x = x + chosen[c][r:r + 1, :] * rows_of[r]
        mean = total(x) * (1.0 / features)
        spread = total(x * x) * (1.0 / features) - mean * mean
        slots.append((x - mean) * lax.rsqrt(spread + NORM_EPS) * gain2)
    slots16 = jnp.concatenate(slots, axis=0).astype(BF16)
    msg5[...] = slots16

    send(5, "tp", tp_peers, msg5, rec5, False)
    rec5[tp] = slots16
    for copy in loads[18:]:
        copy.wait()
    arrive(5, rec5)
    rows_c = capacity * n_ep
    slot_count = capacity * n_tp
    for t in range(n_tp):
        wide_s[t * rows_c:(t + 1) * rows_c, :] = rec5[t].astype(F32)
    x = jnp.concatenate(
        [wide_s[pl.ds(e, slot_count, n_ep), :].astype(BF16) for e in range(n_ep)], axis=1
    )
    gate = jnp.dot(x, eg_v[0], preferred_element_type=F32)
    up = jnp.dot(x, eu_v[0], preferred_element_type=F32)
    active = (jax.nn.silu(gate) * up).astype(BF16)
    down = jnp.dot(active, ed_v[0], preferred_element_type=F32)
    for e in range(n_ep):
        wide_s[pl.ds(e, slot_count, n_ep), :] = down[:, e * LANES:(e + 1) * LANES]
    for t in range(n_tp):
        msg6[t] = wide_s[t * rows_c:(t + 1) * rows_c, :].astype(BF16)
    send(6, "tp", tp_peers, msg6, rec6, True)
    rec6[tp] = msg6[tp]
    slot_s[...] = jnp.zeros_like(slot_s)
    arrive(6, rec6)
    done = rec6[0].astype(F32)
    for t in range(1, n_tp):
        done = done + rec6[t].astype(F32)
    for c in range(capacity):
        slot_s[pl.ds(c, n_ep, SUB), :] = done[c * n_ep:(c + 1) * n_ep]
    for e in range(n_ep):
        msg7[e] = slot_s[e * SUB:(e + 1) * SUB, :].astype(BF16)

    send(7, "ep", ep_peers, msg7, rec7, True, capacity)
    rec7[ep] = msg7[ep]
    arrive(7, rec7, capacity)
    returned = jnp.concatenate([rec7[e].astype(F32) for e in range(n_ep)], axis=0).astype(BF16)
    lhs = jnp.concatenate(
        [weight_high.astype(F32), weight_mid.astype(F32), weight_low.astype(F32)], axis=0
    )[:, :SUB * n_ep].astype(BF16)
    moe = jnp.dot(lhs, returned, preferred_element_type=F32)
    moe = moe[0:SUB] + moe[SUB:2 * SUB] + moe[2 * SUB:3 * SUB]
    layer16 = (stream + moe).astype(BF16)
    msg8[...] = layer16
    send(8, "tp", tp_peers, msg8, rec8, False, seq_local)
    rec8[tp] = layer16
    arrive(8, rec8, seq_local)
    finished = jnp.concatenate([rec8[t].astype(F32) for t in range(n_tp)], axis=0).astype(BF16)
    c8 = iota((seqs, SUB * n_tp), 1)
    unpick = (c8 // SUB) * seq_local + c8 % SUB == iota((seqs, SUB * n_tp), 0)
    unpick = unpick & (c8 % SUB < seq_local)
    out_ref[...] = jnp.dot(unpick.astype(BF16), finished, preferred_element_type=F32).astype(BF16)

    used_rows = (None, q_rows, None, seq_local, seq_local, None, None, capacity, seq_local, None)
    for phase, target in enumerate((rec0, rec1, rec2, rec3, rec4, rec5, rec6, rec7, rec8, recv)):
        settle(send_sem.at[phase], target, used_rows[phase])


def write_out(*refs):
    *refs, sem = refs
    count = len(refs) // 2
    copies = [pltpu.make_async_copy(refs[i], refs[count + i], sem.at[i]) for i in range(count)]
    for copy in copies:
        copy.start()
    for copy in copies:
        copy.wait()


def solution(mesh):
    n_ep = mesh.shape["ep"]
    n_tp = mesh.shape["tp"]

    def on_device(*args):
        (
            tokens, first_gain, w_query, w_key, w_value, w_outgate, w_input, w_forget,
            input_bias, forget_bias, head_gain, w_project, cell_state, norm_state, max_state,
            second_gain, routes, route_weight, expert_gate, expert_up, expert_down,
        ) = args
        seq_local = tokens.shape[0] // n_ep
        key_size, value_size = cell_state.shape[2], cell_state.shape[3]
        capacity = 2
        operands = (
            tokens, first_gain.reshape(n_ep, LANES), w_query, w_key, w_value, w_outgate,
            w_input.T, w_forget.T, input_bias.reshape(1, -1), forget_bias.reshape(1, -1),
            head_gain.reshape(-1, LANES), w_project, cell_state, norm_state, max_state.T,
            second_gain.reshape(n_ep, LANES), routes.T, route_weight.T,
            expert_gate, expert_up, expert_down,
        )
        results = (
            jax.ShapeDtypeStruct(tokens.shape, BF16),
            jax.ShapeDtypeStruct(cell_state.shape, F32),
            jax.ShapeDtypeStruct(norm_state.shape, F32),
            jax.ShapeDtypeStruct((1, seq_local), F32),
        )
        hbm = pl.BlockSpec(memory_space=pltpu.HBM)
        vmem = pl.BlockSpec(memory_space=pltpu.VMEM)
        rows8 = max(SUB * n_ep, LANES)
        vt = value_size // LANES

        def pair(shape_out, shape_in, dtype):
            return [pltpu.VMEM(shape_out, dtype), pltpu.VMEM(shape_in, dtype)]

        messages = (
            pair((2, rows8), (n_ep, 2, rows8), F32)
            + pair((n_ep, 2 * SUB, value_size), (n_ep, 2 * SUB, value_size), BF16)
            + pair((n_ep, SUB, 2 * key_size), (n_ep, SUB, 2 * key_size), F32)
            + pair((vt * SUB, LANES), (n_ep, vt * SUB, LANES), BF16)
            + pair((n_tp, SUB, LANES), (n_tp, SUB, LANES), BF16)
            + pair((SUB, LANES), (n_ep, SUB, LANES), BF16)
            + pair((capacity * n_ep, LANES), (n_tp, capacity * n_ep, LANES), BF16)
            + pair((n_tp, capacity * n_ep, LANES), (n_tp, capacity * n_ep, LANES), BF16)
            + pair((n_ep, SUB, LANES), (n_ep, SUB, LANES), BF16)
            + pair((SUB, LANES), (n_tp, SUB, LANES), BF16)
        )
        held = pl.pallas_call(
            functools.partial(kernel, n_ep, n_tp, seq_local, key_size, value_size),
            out_shape=tuple(pltpu.VMEM(r.shape, r.dtype) for r in results),
            in_specs=[hbm] * len(operands),
            out_specs=(vmem, vmem, vmem, vmem),
            scratch_shapes=[pltpu.VMEM(a.shape, a.dtype) for a in operands]
            + messages
            + [
                pltpu.VMEM((rows8, LANES), F32),
                pltpu.VMEM((2 * vt, rows8, LANES), F32),
                pltpu.VMEM((n_ep, rows8), F32),
                pltpu.VMEM((SUB * n_ep, LANES), F32),
                pltpu.VMEM((n_tp * capacity * n_ep, LANES), F32),
                pltpu.SemaphoreType.DMA((len(operands),)),
                pltpu.SemaphoreType.DMA((10,)),
                pltpu.SemaphoreType.DMA((10,)),
                pltpu.SemaphoreType.REGULAR((3,)),
            ],
            compiler_params=pltpu.CompilerParams(
                collective_id=0, has_side_effects=True
            ),
        )(*operands)
        out, new_cell, new_norm, new_max = pl.pallas_call(
            write_out,
            out_shape=results,
            in_specs=[pl.BlockSpec(memory_space=pl.ANY)] * len(results),
            out_specs=(hbm,) * len(results),
            scratch_shapes=[pltpu.SemaphoreType.DMA((len(results),))],
            compiler_params=pltpu.CompilerParams(vmem_limit_bytes=1024 * 1024),
        )(*held)
        return out, new_cell, new_norm, new_max.T

    placed = (
        P("grp", "ep"), P(), P("ep", "tp"), P("ep", "tp"), P("ep", "tp"), P("ep", "tp"),
        P(), P(), P(), P(), P(), P("tp", "ep"),
        P(("grp", "ep"), "tp", None, None), P(("grp", "ep"), "tp", None), P(("grp", "ep"), "tp"),
        P(), P("grp", None), P("grp", None),
        P("ep", None, "tp"), P("ep", None, "tp"), P("ep", "tp", None),
    )
    return jax.shard_map(
        on_device,
        mesh=mesh,
        in_specs=placed,
        out_specs=(
            P("grp", "ep"),
            P(("grp", "ep"), "tp", None, None),
            P(("grp", "ep"), "tp", None),
            P(("grp", "ep"), "tp"),
        ),
        check_vma=False,
    )
```

```python
import functools

import jax
import jax.numpy as jnp
from jax import lax
from jax.experimental import pallas as pl
from jax.experimental.pallas import tpu as pltpu
from jax.sharding import PartitionSpec as P

NORM_EPS = 1e-05
HEAD_EPS = 1e-06
F32 = jnp.float32
BF16 = jnp.bfloat16
LANES = 128
SUB = 8


def iota(shape, dim):
    return lax.broadcasted_iota(jnp.int32, shape, dim)


def total(x):
    return jnp.sum(jnp.sum(x, axis=1, keepdims=True), axis=0, keepdims=True)


def far_first(n):
    order = [n // 2]
    for d in range(1, n // 2):
        order += [n // 2 + d, n // 2 - d]
    if n % 2 == 0:
        return [d for d in order if 0 < d < n]
    return list(range(1, n))


def kernel(
    n_ep, n_tp, seq_local, key_size, value_size,
    tokens_h, gain1_h, wq_h, wk_h, wv_h, wo_h, win_h, wfg_h, ib_h, fb_h, hg_h, wp_h,
    cell_h, norm_h, max_h, gain2_h, routes_h, rw_h, eg_h, eu_h, ed_h,
    out_ref, ncell_ref, nnorm_ref, nmax_ref,
    tokens_v, gain1_v, wq_v, wk_v, wv_v, wo_v, win_v, wfg_v, ib_v, fb_v, hg_v, wp_v,
    cell_v, norm_v, max_v, gain2_v, routes_v, rw_v, eg_v, eu_v, ed_v,
    msg0, rec0, msgv, recv, msg1, rec1, msg2, rec2, msg3, rec3, msg4, rec4, msg5, rec5, msg6, rec6, msg7, rec7, msg8, rec8,
    table, t8_s, part_s, sum_s, slot_s, wide_s,
    load_sem, send_sem, recv_sem, known_sem, stat_send, stat_recv,
):
    ep = lax.axis_index("ep")
    tp = lax.axis_index("tp")
    barrier = pltpu.get_barrier_semaphore()
    rec7[...] = jnp.zeros_like(rec7)
    rec8[...] = jnp.zeros_like(rec8)
    table[...] = jnp.zeros_like(table)
    ep_peers = [lax.rem(ep + d, n_ep) for d in far_first(n_ep)]
    tp_peers = [lax.rem(tp + d, n_tp) for d in far_first(n_tp)]
    def tell(sem, reach):
        for d in (reach, n_tp - reach):
            peer = lax.rem(tp + d, n_tp)
            pl.semaphore_signal(sem, inc=1, device_id={"tp": peer}, device_id_type=pl.DeviceIdType.MESH)

    tell(barrier, 1)

    sources = (
        tokens_h, gain1_h, wq_h, wk_h, wv_h, wo_h, win_h, wfg_h, ib_h, fb_h, hg_h, wp_h,
        cell_h, norm_h, max_h, gain2_h, routes_h, rw_h, eg_h, eu_h, ed_h,
    )
    targets = (
        tokens_v, gain1_v, wq_v, wk_v, wv_v, wo_v, win_v, wfg_v, ib_v, fb_v, hg_v, wp_v,
        cell_v, norm_v, max_v, gain2_v, routes_v, rw_v, eg_v, eu_v, ed_v,
    )
    loads = [
        pltpu.make_async_copy(s, t, load_sem.at[i]) for i, (s, t) in enumerate(zip(sources, targets))
    ]
    for copy in loads:
        copy.start()

    def send(phase, axis, peers, source, target, each, used=None):
        me = ep if axis == "ep" else tp
        used = pl.ds(0, target.shape[1] if used is None else used)
        for peer in peers:
            pltpu.make_async_remote_copy(
                src_ref=source.at[peer, used] if each else source.at[used],
                dst_ref=target.at[me, used],
                send_sem=send_sem.at[phase],
                recv_sem=recv_sem.at[phase],
                device_id={axis: peer},
                device_id_type=pl.DeviceIdType.MESH,
            ).start()

    def settle(sem, target, used):
        used = target.shape[1] if used is None else used
        others = target.at[pl.ds(0, target.shape[0] - 1), pl.ds(0, used)]
        pltpu.make_async_copy(others, others, sem).wait()

    def arrive(phase, target, used=None):
        settle(recv_sem.at[phase], target, used)

    rows8 = max(SUB * n_ep, LANES)
    seqs = n_ep * seq_local
    features = n_ep * LANES
    nt = (((1,), (1,)), ((), ()))
    sub = iota((SUB, LANES), 0)
    lane = iota((SUB, LANES), 1)
    kt = key_size // LANES
    vt = value_size // LANES

    for copy in loads[:6]:
        copy.wait()
    r8 = iota((rows8, seqs), 0)
    pick = ((r8 // SUB) * seq_local + r8 % SUB == iota((rows8, seqs), 1)) & (r8 % SUB < seq_local)
    t8 = jnp.dot(pick.astype(BF16), tokens_v[...], preferred_element_type=F32)
    t8_s[...] = t8
    wide_lane = iota((rows8, LANES), 1)
    row_sum = jnp.sum(t8, axis=1, keepdims=True)
    row_square = jnp.sum(t8 * t8, axis=1, keepdims=True)
    stats = jnp.where(wide_lane == 0, row_sum, jnp.where(wide_lane == 1, row_square, 0.0)).T
    msg0[...] = stats[0:2]
    gain_here = gain1_v[pl.ds(ep, 1), :]
    gain_high = gain_here.astype(BF16).astype(F32)
    kind = iota((rows8, LANES), 0) % SUB
    centred = (t8 - row_sum * (1.0 / LANES)) * gain_here
    left = jnp.where(
        kind == seq_local, gain_high, jnp.where(kind == seq_local + 1, gain_here - gain_high, centred)
    ).astype(BF16)
    at = 0
    for w in (wv_v, wo_v):
        part = jnp.dot(left, w[...], preferred_element_type=F32)
        for j in range(vt):
            part_s[at] = part[:, j * LANES:(j + 1) * LANES]
            at += 1
    for j in range(2 * vt):
        gain_term = part_s[j, pl.ds(seq_local, 1), :] + part_s[j, pl.ds(seq_local + 1, 1), :]
        term_high = gain_term.astype(BF16).astype(F32)
        part_s[j, pl.ds(seq_local, n_ep, SUB), :] = jnp.broadcast_to(term_high, (n_ep, LANES))
        part_s[j, pl.ds(seq_local + 1, n_ep, SUB), :] = jnp.broadcast_to(
            gain_term - term_high, (n_ep, LANES)
        )
    for p in range(n_ep):
        rows = slice(p * SUB, (p + 1) * SUB)
        for j in range(vt):
            msgv[p, :, j * LANES:(j + 1) * LANES] = jnp.concatenate(
                [part_s[j, rows, :], part_s[vt + j, rows, :]], axis=0
            ).astype(BF16)

    @pl.when(ep == 0)
    def _():
        pl.semaphore_wait(barrier, 2)

    @pl.when(ep > 0)
    def _():
        pl.semaphore_wait(barrier, 3)

    above = lax.rem(ep + 1, n_ep)

    @pl.when(ep < n_ep - 1)
    def _():
        pl.semaphore_signal(barrier, inc=1, device_id={"ep": above}, device_id_type=pl.DeviceIdType.MESH)

    rounds = [1]
    while 2 * rounds[-1] < n_tp // 2:
        rounds.append(2 * rounds[-1])
    def statistics_to(peer):
        return pltpu.make_async_remote_copy(
            src_ref=msg0, dst_ref=rec0.at[ep], send_sem=stat_send.at[peer], recv_sem=stat_recv.at[ep],
            device_id={"ep": peer}, device_id_type=pl.DeviceIdType.MESH,
        )

    def terms_to(peer):
        return pltpu.make_async_remote_copy(
            src_ref=msgv.at[peer], dst_ref=recv.at[ep], send_sem=send_sem.at[9], recv_sem=recv_sem.at[9],
            device_id={"ep": peer}, device_id_type=pl.DeviceIdType.MESH,
        )

    table_up = pltpu.make_async_remote_copy(
        src_ref=table, dst_ref=table, send_sem=send_sem.at[0], recv_sem=recv_sem.at[0],
        device_id={"ep": above}, device_id_type=pl.DeviceIdType.MESH,
    )
    for make in (statistics_to, terms_to):
        for d in far_first(n_ep):
            @pl.when(ep >= d)
            def _(make=make, d=d):
                make(lax.rem(ep + n_ep - d, n_ep)).start()
    recv[ep] = msgv[ep]

    tell(known_sem.at[0], rounds[0])

    for copy in loads[6:18]:
        copy.wait()
    here = pl.ds(pl.multiple_of(ep * LANES, LANES), LANES)
    gate_w = jnp.zeros((SUB, LANES), F32)
    for row, source in enumerate((win_v, wfg_v)):
        head = (iota((SUB, n_tp), 1) == tp) & (iota((SUB, n_tp), 0) == row)
        gate_w = gate_w + jnp.dot(head.astype(BF16), source[:, here], preferred_element_type=F32)
    gate_w = gate_w.astype(BF16)
    at_head = iota((1, n_tp), 1) == tp
    input_bias = jnp.sum(jnp.where(at_head, ib_v[...], 0.0), axis=1, keepdims=True)
    forget_bias = jnp.sum(jnp.where(at_head, fb_v[...], 0.0), axis=1, keepdims=True)

    top = routes_v.shape[0]
    own_row = iota((SUB, seqs), 1) == tp * seq_local + iota((SUB, seqs), 0)
    own_row = own_row & (iota((SUB, seqs), 0) < seq_local)
    routed = jnp.zeros((SUB, LANES), F32)
    combine = jnp.zeros((SUB, LANES), F32)
    for k in range(top):
        named = jnp.sum(
            jnp.where(own_row, routes_v[k:k + 1, :].astype(F32) + 1.0, 0.0), axis=1, keepdims=True
        )
        weight = jnp.sum(jnp.where(own_row, rw_v[k:k + 1, :], 0.0), axis=1, keepdims=True)
        match = jnp.abs(named - 1.0 - (lane // SUB).astype(F32)) < 0.5
        routed = routed + jnp.where(match, 1.0, 0.0)
        combine = combine + jnp.where(match, weight, 0.0)
    before = (iota((SUB, SUB), 1) < iota((SUB, SUB), 0)).astype(BF16)
    running = jnp.dot(before, routed.astype(BF16), preferred_element_type=F32)
    placed = jnp.where((routed > 0.5) & (jnp.abs(running - (lane % SUB).astype(F32)) < 0.5), 1.0, 0.0)
    slot_weight = placed * combine
    weight_high = slot_weight.astype(BF16)
    rest = slot_weight - weight_high.astype(F32)
    weight_mid = rest.astype(BF16)
    weight_low = (rest - weight_mid.astype(F32)).astype(BF16)
    capacity = 2
    chosen = [
        jnp.sum(jnp.where(lane == ep * SUB + c, placed, 0.0), axis=1, keepdims=True) for c in range(capacity)
    ]

    if len(rounds) > 1:
        pl.semaphore_wait(known_sem.at[0], 2)
        tell(known_sem.at[1], rounds[1])
    @pl.when(ep > 0)
    def _():
        table_up.wait_recv()

    table[ep] = msg0[...]
    for e in range(1, n_ep):
        @pl.when(e > ep)
        def _(e=e):
            pltpu.make_async_copy(rec0.at[e], rec0.at[e], stat_recv.at[e]).wait()

            @pl.when(e == ep + 1)
            def _():
                table_up.start()

            terms_to(e).start()

    stat = jnp.zeros((2, rows8), F32)
    for e in range(n_ep):
        theirs = jnp.where(e <= ep, table[e], rec0[e])
        stat = stat + theirs
        sum_s[e:e + 1, :] = theirs[0:1]
    stat8 = jnp.where(sub == 0, stat[0:1], jnp.where(sub == 1, stat[1:2], 0.0))
    column = stat8.T
    mean = column[:, 0:1] * (1.0 / features)
    spread = column[:, 1:2] * (1.0 / features) - mean * mean
    normed = ((t8_s[...] - mean) * lax.rsqrt(spread + NORM_EPS) * gain_here).astype(BF16)
    gate_rows = lax.dot_general(gate_w, normed, nt, preferred_element_type=F32)
    for j, w in enumerate((wq_v, wk_v)):
        part = jnp.dot(normed, w[...], preferred_element_type=F32)
        part = jnp.where(kind == seq_local, gate_rows[j:j + 1], part)
        for p in range(n_ep):
            msg1[p, :, j * LANES:(j + 1) * LANES] = part[p * SUB:(p + 1) * SUB]
    q_rows = seq_local + 1
    send(1, "ep", ep_peers, msg1, rec1, True, q_rows)
    rec1[ep] = msg1[ep]

    mine = (lane == ep * SUB + sub) & (sub < seq_local)
    own_mean = jnp.sum(jnp.where(mine, stat[0:1], 0.0), axis=1, keepdims=True) * (1.0 / features)
    own_square = jnp.sum(jnp.where(mine, stat[1:2], 0.0), axis=1, keepdims=True) * (1.0 / features)
    own_inv = lax.rsqrt(own_square - own_mean * own_mean + NORM_EPS)
    off = lax.dot_general(
        jnp.where(mine, 1.0, 0.0), sum_s[...], nt,
        preferred_element_type=F32, precision=lax.Precision.HIGHEST,
    ) * (1.0 / LANES) - own_mean
    if len(rounds) > 2:
        pl.semaphore_wait(known_sem.at[1], 2)
        tell(known_sem.at[2], rounds[2])
    arrive(9, recv)
    for e in range(n_ep):
        arrived = recv[e].astype(F32)
        for j in range(vt):
            piece = arrived[:, j * LANES:(j + 1) * LANES]
            part_s[j, e * SUB:(e + 1) * SUB, :] = piece[:SUB]
            part_s[vt + j, e * SUB:(e + 1) * SUB, :] = piece[SUB:]
    rest_of = []
    for j in range(2 * vt):
        acc = part_s[j, 0:SUB, :]
        for e in range(1, n_ep):
            acc = acc + part_s[j, e * SUB:(e + 1) * SUB, :]
        gain_terms = part_s[j, pl.ds(seq_local, n_ep, SUB), :] + part_s[j, pl.ds(seq_local + 1, n_ep, SUB), :]
        acc = acc + jnp.dot(
            off, gain_terms, preferred_element_type=F32, precision=lax.Precision.HIGHEST
        )
        rest_of.append(jnp.where(sub < seq_local, acc * own_inv, 0.0).astype(BF16).astype(F32))
    value = jnp.concatenate(rest_of[:vt], axis=1)
    outgate = jax.nn.sigmoid(jnp.concatenate(rest_of[vt:], axis=1))
    max8 = jnp.zeros((SUB, LANES), F32)
    for i in range(seq_local):
        max8 = jnp.where(sub == i, max_v[:, i:i + 1], max8)
    head_gain = jnp.concatenate([hg_v[pl.ds(tp * vt + j, 1), :] for j in range(vt)], axis=1)
    wide_p = jnp.concatenate([wp_v[j * LANES:(j + 1) * LANES, :] for j in range(vt)], axis=1)

    arrive(1, rec1, q_rows)
    sums = rec1[0]
    for e in range(1, n_ep):
        sums = sums + rec1[e]
    in8 = jnp.sum(
        jnp.where(mine, sums[seq_local:seq_local + 1, :LANES], 0.0), axis=1, keepdims=True
    ) + input_bias
    fg8 = jnp.sum(
        jnp.where(mine, sums[seq_local:seq_local + 1, LANES:2 * LANES], 0.0), axis=1, keepdims=True
    ) + forget_bias
    carried = jnp.minimum(fg8, 0.0) - jnp.log1p(jnp.exp(-jnp.abs(fg8))) + max8
    new_max = jnp.maximum(carried, in8)
    keep = jnp.exp(carried - new_max)
    admit = jnp.exp(in8 - new_max)
    across = jnp.sum(jnp.where(sub == iota((SUB, LANES), 1), new_max, 0.0), axis=0, keepdims=True)
    nmax_ref[...] = across[:, :seq_local]
    sums = jnp.where(iota((SUB, 2 * LANES), 0) < seq_local, sums, 0.0)
    query = sums[:, :LANES].astype(BF16).astype(F32) * key_size ** (-0.5)
    admitted = admit * sums[:, LANES:2 * LANES].astype(BF16).astype(F32)
    query_t = query.T
    admitted_t = admitted.T
    sub_wide = iota((SUB, value_size), 0)
    readout = jnp.zeros((SUB, value_size), F32)
    for i in range(seq_local):
        nnorm_ref[i] = keep[i:i + 1] * norm_v[i] + admitted[i:i + 1]
        new_cell = keep[i:i + 1, 0:1] * cell_v[i, 0] + admitted_t[:, i:i + 1] * value[i:i + 1, :]
        ncell_ref[i, 0] = new_cell
        read = jnp.sum(query_t[:, i:i + 1] * new_cell, axis=0, keepdims=True)
        readout = jnp.where(sub_wide == i, read, readout)
    head_mean = jnp.mean(readout, axis=1, keepdims=True)
    spread_out = readout - head_mean
    head_var = jnp.mean(spread_out * spread_out, axis=1, keepdims=True)
    mixed = spread_out * lax.rsqrt(head_var + HEAD_EPS) * head_gain * outgate
    mixed = jnp.concatenate([mixed[:, j * LANES:(j + 1) * LANES] for j in range(vt)], axis=0).astype(BF16)
    msg2[...] = mixed

    send(2, "ep", ep_peers, msg2, rec2, False)
    rec2[ep] = mixed
    arrive(2, rec2)
    terms = jnp.dot(
        rec2[...].reshape(n_ep * vt * SUB, LANES), wide_p, preferred_element_type=F32
    )
    for p in range(n_ep):
        term = jnp.zeros((SUB, LANES), F32)
        for j in range(vt):
            start = (p * vt + j) * SUB
            term = term + terms[start:start + SUB, j * LANES:(j + 1) * LANES]
        msg3[p] = term.astype(BF16)
    last = len(rounds) - 1
    pl.semaphore_wait(known_sem.at[last], 2)
    send(3, "tp", tp_peers, msg3, rec3, True, seq_local)
    rec3[tp] = msg3[tp]
    arrive(3, rec3, seq_local)
    mixer = rec3[0].astype(F32)
    for t in range(1, n_tp):
        mixer = mixer + rec3[t].astype(F32)
    mixer = jnp.where(sub < seq_local, mixer, 0.0)
    stream16 = (t8_s[pl.ds(pl.multiple_of(tp * SUB, SUB), SUB), :] + mixer).astype(BF16)
    stream = stream16.astype(F32)
    msg4[...] = stream16

    send(4, "ep", ep_peers, msg4, rec4, False, seq_local)
    rec4[ep] = stream16
    gain2 = gain2_v[...]
    arrive(4, rec4, seq_local)
    for e in range(n_ep):
        slot_s[e * SUB:(e + 1) * SUB, :] = rec4[e].astype(F32)
    rows_of = [slot_s[pl.ds(r, n_ep, SUB), :] for r in range(seq_local)]
    slots = []
    for c in range(capacity):
        x = chosen[c][0:1, :] * rows_of[0]
        for r in range(1, seq_local):
            x = x + chosen[c][r:r + 1, :] * rows_of[r]
        mean = total(x) * (1.0 / features)
        spread = total(x * x) * (1.0 / features) - mean * mean
        slots.append((x - mean) * lax.rsqrt(spread + NORM_EPS) * gain2)
    slots16 = jnp.concatenate(slots, axis=0).astype(BF16)
    msg5[...] = slots16

    send(5, "tp", tp_peers, msg5, rec5, False)
    rec5[tp] = slots16
    for copy in loads[18:]:
        copy.wait()
    arrive(5, rec5)
    rows_c = capacity * n_ep
    slot_count = capacity * n_tp
    for t in range(n_tp):
        wide_s[t * rows_c:(t + 1) * rows_c, :] = rec5[t].astype(F32)
    x = jnp.concatenate(
        [wide_s[pl.ds(e, slot_count, n_ep), :].astype(BF16) for e in range(n_ep)], axis=1
    )
    gate = jnp.dot(x, eg_v[0], preferred_element_type=F32)
    up = jnp.dot(x, eu_v[0], preferred_element_type=F32)
    active = (jax.nn.silu(gate) * up).astype(BF16)
    down = jnp.dot(active, ed_v[0], preferred_element_type=F32)
    for e in range(n_ep):
        wide_s[pl.ds(e, slot_count, n_ep), :] = down[:, e * LANES:(e + 1) * LANES]
    for t in range(n_tp):
        msg6[t] = wide_s[t * rows_c:(t + 1) * rows_c, :].astype(BF16)
    send(6, "tp", tp_peers, msg6, rec6, True)
    rec6[tp] = msg6[tp]
    slot_s[...] = jnp.zeros_like(slot_s)
    arrive(6, rec6)
    done = rec6[0].astype(F32)
    for t in range(1, n_tp):
        done = done + rec6[t].astype(F32)
    for c in range(capacity):
        slot_s[pl.ds(c, n_ep, SUB), :] = done[c * n_ep:(c + 1) * n_ep]
    for e in range(n_ep):
        msg7[e] = slot_s[e * SUB:(e + 1) * SUB, :].astype(BF16)

    send(7, "ep", ep_peers, msg7, rec7, True, capacity)
    rec7[ep] = msg7[ep]
    arrive(7, rec7, capacity)
    returned = jnp.concatenate([rec7[e].astype(F32) for e in range(n_ep)], axis=0).astype(BF16)
    lhs = jnp.concatenate(
        [weight_high.astype(F32), weight_mid.astype(F32), weight_low.astype(F32)], axis=0
    )[:, :SUB * n_ep].astype(BF16)
    moe = jnp.dot(lhs, returned, preferred_element_type=F32)
    moe = moe[0:SUB] + moe[SUB:2 * SUB] + moe[2 * SUB:3 * SUB]
    layer16 = (stream + moe).astype(BF16)
    msg8[...] = layer16
    send(8, "tp", tp_peers, msg8, rec8, False, seq_local)
    rec8[tp] = layer16
    arrive(8, rec8, seq_local)
    finished = jnp.concatenate([rec8[t].astype(F32) for t in range(n_tp)], axis=0).astype(BF16)
    c8 = iota((seqs, SUB * n_tp), 1)
    unpick = (c8 // SUB) * seq_local + c8 % SUB == iota((seqs, SUB * n_tp), 0)
    unpick = unpick & (c8 % SUB < seq_local)
    out_ref[...] = jnp.dot(unpick.astype(BF16), finished, preferred_element_type=F32).astype(BF16)

    @pl.when(ep < n_ep - 1)
    def _():
        table_up.wait_send()

    for e in range(n_ep - 1):
        @pl.when(e < ep)
        def _(e=e):
            pltpu.make_async_copy(msg0, msg0, stat_send.at[e]).wait()

    used_rows = (q_rows, None, seq_local, seq_local, None, None, capacity, seq_local, None)
    for phase, target in enumerate((rec1, rec2, rec3, rec4, rec5, rec6, rec7, rec8, recv), 1):
        settle(send_sem.at[phase], target, used_rows[phase - 1])


def write_out(*refs):
    *refs, sem = refs
    count = len(refs) // 2
    copies = [pltpu.make_async_copy(refs[i], refs[count + i], sem.at[i]) for i in range(count)]
    for copy in copies:
        copy.start()
    for copy in copies:
        copy.wait()


def solution(mesh):
    n_ep = mesh.shape["ep"]
    n_tp = mesh.shape["tp"]

    def on_device(*args):
        (
            tokens, first_gain, w_query, w_key, w_value, w_outgate, w_input, w_forget,
            input_bias, forget_bias, head_gain, w_project, cell_state, norm_state, max_state,
            second_gain, routes, route_weight, expert_gate, expert_up, expert_down,
        ) = args
        seq_local = tokens.shape[0] // n_ep
        key_size, value_size = cell_state.shape[2], cell_state.shape[3]
        capacity = 2
        operands = (
            tokens, first_gain.reshape(n_ep, LANES), w_query, w_key, w_value, w_outgate,
            w_input.T, w_forget.T, input_bias.reshape(1, -1), forget_bias.reshape(1, -1),
            head_gain.reshape(-1, LANES), w_project, cell_state, norm_state, max_state.T,
            second_gain.reshape(n_ep, LANES), routes.T, route_weight.T,
            expert_gate, expert_up, expert_down,
        )
        results = (
            jax.ShapeDtypeStruct(tokens.shape, BF16),
            jax.ShapeDtypeStruct(cell_state.shape, F32),
            jax.ShapeDtypeStruct(norm_state.shape, F32),
            jax.ShapeDtypeStruct((1, seq_local), F32),
        )
        hbm = pl.BlockSpec(memory_space=pltpu.HBM)
        vmem = pl.BlockSpec(memory_space=pltpu.VMEM)
        rows8 = max(SUB * n_ep, LANES)
        vt = value_size // LANES

        def pair(shape_out, shape_in, dtype):
            return [pltpu.VMEM(shape_out, dtype), pltpu.VMEM(shape_in, dtype)]

        messages = (
            pair((2, rows8), (n_ep, 2, rows8), F32)
            + pair((n_ep, 2 * SUB, value_size), (n_ep, 2 * SUB, value_size), BF16)
            + pair((n_ep, SUB, 2 * key_size), (n_ep, SUB, 2 * key_size), F32)
            + pair((vt * SUB, LANES), (n_ep, vt * SUB, LANES), BF16)
            + pair((n_tp, SUB, LANES), (n_tp, SUB, LANES), BF16)
            + pair((SUB, LANES), (n_ep, SUB, LANES), BF16)
            + pair((capacity * n_ep, LANES), (n_tp, capacity * n_ep, LANES), BF16)
            + pair((n_tp, capacity * n_ep, LANES), (n_tp, capacity * n_ep, LANES), BF16)
            + pair((n_ep, SUB, LANES), (n_ep, SUB, LANES), BF16)
            + pair((SUB, LANES), (n_tp, SUB, LANES), BF16)
        )
        held = pl.pallas_call(
            functools.partial(kernel, n_ep, n_tp, seq_local, key_size, value_size),
            out_shape=tuple(pltpu.VMEM(r.shape, r.dtype) for r in results),
            in_specs=[hbm] * len(operands),
            out_specs=(vmem, vmem, vmem, vmem),
            scratch_shapes=[pltpu.VMEM(a.shape, a.dtype) for a in operands]
            + messages
            + [
                pltpu.VMEM((n_ep, 2, rows8), F32),
                pltpu.VMEM((rows8, LANES), F32),
                pltpu.VMEM((2 * vt, rows8, LANES), F32),
                pltpu.VMEM((n_ep, rows8), F32),
                pltpu.VMEM((SUB * n_ep, LANES), F32),
                pltpu.VMEM((n_tp * capacity * n_ep, LANES), F32),
                pltpu.SemaphoreType.DMA((len(operands),)),
                pltpu.SemaphoreType.DMA((10,)),
                pltpu.SemaphoreType.DMA((10,)),
                pltpu.SemaphoreType.REGULAR((3,)),
                pltpu.SemaphoreType.DMA((n_ep,)),
                pltpu.SemaphoreType.DMA((n_ep,)),
            ],
            compiler_params=pltpu.CompilerParams(
                collective_id=0, has_side_effects=True
            ),
        )(*operands)
        out, new_cell, new_norm, new_max = pl.pallas_call(
            write_out,
            out_shape=results,
            in_specs=[pl.BlockSpec(memory_space=pl.ANY)] * len(results),
            out_specs=(hbm,) * len(results),
            scratch_shapes=[pltpu.SemaphoreType.DMA((len(results),))],
            compiler_params=pltpu.CompilerParams(vmem_limit_bytes=1024 * 1024),
        )(*held)
        return out, new_cell, new_norm, new_max.T

    placed = (
        P("grp", "ep"), P(), P("ep", "tp"), P("ep", "tp"), P("ep", "tp"), P("ep", "tp"),
        P(), P(), P(), P(), P(), P("tp", "ep"),
        P(("grp", "ep"), "tp", None, None), P(("grp", "ep"), "tp", None), P(("grp", "ep"), "tp"),
        P(), P("grp", None), P("grp", None),
        P("ep", None, "tp"), P("ep", None, "tp"), P("ep", "tp", None),
    )
    return jax.shard_map(
        on_device,
        mesh=mesh,
        in_specs=placed,
        out_specs=(
            P("grp", "ep"),
            P(("grp", "ep"), "tp", None, None),
            P(("grp", "ep"), "tp", None),
            P(("grp", "ep"), "tp"),
        ),
        check_vma=False,
    )
```

```python
import functools

import jax
import jax.numpy as jnp
from jax import lax
from jax.experimental import pallas as pl
from jax.experimental.pallas import tpu as pltpu
from jax.sharding import PartitionSpec as P

NORM_EPS = 1e-05
HEAD_EPS = 1e-06
F32 = jnp.float32
BF16 = jnp.bfloat16
LANES = 128
SUB = 8


def iota(shape, dim):
    return lax.broadcasted_iota(jnp.int32, shape, dim)


def total(x):
    return jnp.sum(jnp.sum(x, axis=1, keepdims=True), axis=0, keepdims=True)


def far_first(n):
    order = [n // 2]
    for d in range(1, n // 2):
        order += [n // 2 + d, n // 2 - d]
    if n % 2 == 0:
        return [d for d in order if 0 < d < n]
    return list(range(1, n))


def kernel(
    n_ep, n_tp, seq_local, key_size, value_size,
    tokens_h, gain1_h, wq_h, wk_h, wv_h, wo_h, win_h, wfg_h, ib_h, fb_h, hg_h, wp_h,
    cell_h, norm_h, max_h, gain2_h, routes_h, rw_h, eg_h, eu_h, ed_h,
    out_ref, ncell_ref, nnorm_ref, nmax_ref,
    tokens_v, gain1_v, wq_v, wk_v, wv_v, wo_v, win_v, wfg_v, ib_v, fb_v, hg_v, wp_v,
    cell_v, norm_v, max_v, gain2_v, routes_v, rw_v, eg_v, eu_v, ed_v,
    msg0, rec0, msgv, recv, msg1, rec1, msg2, rec2, msg3, rec3, msg4, rec4, msg5, rec5, msg6, rec6, msg7, rec7, msg8, rec8,
    table, t8_s, part_s, sum_s, slot_s, wide_s,
    load_sem, send_sem, recv_sem, known_sem, stat_send, stat_recv,
):
    ep = lax.axis_index("ep")
    tp = lax.axis_index("tp")
    barrier = pltpu.get_barrier_semaphore()
    rec7[...] = jnp.zeros_like(rec7)
    rec8[...] = jnp.zeros_like(rec8)
    table[...] = jnp.zeros_like(table)
    ep_peers = [lax.rem(ep + d, n_ep) for d in far_first(n_ep)]
    tp_peers = [lax.rem(tp + d, n_tp) for d in far_first(n_tp)]
    def tell(sem, reach):
        for d in (reach, n_tp - reach):
            peer = lax.rem(tp + d, n_tp)
            pl.semaphore_signal(sem, inc=1, device_id={"tp": peer}, device_id_type=pl.DeviceIdType.MESH)

    tell(barrier, 1)

    sources = (
        tokens_h, gain1_h, wq_h, wk_h, wv_h, wo_h, win_h, wfg_h, ib_h, fb_h, hg_h, wp_h,
        cell_h, norm_h, max_h, gain2_h, routes_h, rw_h, eg_h, eu_h, ed_h,
    )
    targets = (
        tokens_v, gain1_v, wq_v, wk_v, wv_v, wo_v, win_v, wfg_v, ib_v, fb_v, hg_v, wp_v,
        cell_v, norm_v, max_v, gain2_v, routes_v, rw_v, eg_v, eu_v, ed_v,
    )
    loads = [
        pltpu.make_async_copy(s, t, load_sem.at[i]) for i, (s, t) in enumerate(zip(sources, targets))
    ]
    for copy in loads:
        copy.start()

    place = lax.rem(ep + n_ep - 1, n_ep)

    def at_place(q):
        return lax.rem(q + 1, n_ep)

    @pl.when(place == 0)
    def _():
        pl.semaphore_wait(barrier, 2)

    @pl.when((place > 0) & (place < n_ep - 1))
    def _():
        pl.semaphore_wait(barrier, 3)

    @pl.when(place < n_ep - 1)
    def _():
        pl.semaphore_signal(
            barrier, inc=1, device_id={"ep": at_place(place + 1)}, device_id_type=pl.DeviceIdType.MESH
        )

    def send(phase, axis, peers, source, target, each, used=None):
        me = ep if axis == "ep" else tp
        used = pl.ds(0, target.shape[1] if used is None else used)
        for peer in peers:
            pltpu.make_async_remote_copy(
                src_ref=source.at[peer, used] if each else source.at[used],
                dst_ref=target.at[me, used],
                send_sem=send_sem.at[phase],
                recv_sem=recv_sem.at[phase],
                device_id={axis: peer},
                device_id_type=pl.DeviceIdType.MESH,
            ).start()

    def settle(sem, target, used):
        used = target.shape[1] if used is None else used
        others = target.at[pl.ds(0, target.shape[0] - 1), pl.ds(0, used)]
        pltpu.make_async_copy(others, others, sem).wait()

    def arrive(phase, target, used=None):
        settle(recv_sem.at[phase], target, used)

    rows8 = max(SUB * n_ep, LANES)
    seqs = n_ep * seq_local
    features = n_ep * LANES
    nt = (((1,), (1,)), ((), ()))
    sub = iota((SUB, LANES), 0)
    lane = iota((SUB, LANES), 1)
    kt = key_size // LANES
    vt = value_size // LANES

    loads[0].wait()
    r8 = iota((rows8, seqs), 0)
    pick = ((r8 // SUB) * seq_local + r8 % SUB == iota((rows8, seqs), 1)) & (r8 % SUB < seq_local)
    t8 = jnp.dot(pick.astype(BF16), tokens_v[...], preferred_element_type=F32)
    t8_s[...] = t8
    wide_lane = iota((rows8, LANES), 1)
    row_sum = jnp.sum(t8, axis=1, keepdims=True)
    row_square = jnp.sum(t8 * t8, axis=1, keepdims=True)
    stats = jnp.where(wide_lane == 0, row_sum, jnp.where(wide_lane == 1, row_square, 0.0)).T
    msg0[...] = stats[0:2]

    @pl.when(place == n_ep - 1)
    def _():
        pl.semaphore_wait(barrier, 3)

    def statistics_to(q):
        return pltpu.make_async_remote_copy(
            src_ref=msg0, dst_ref=rec0.at[place], send_sem=stat_send.at[q], recv_sem=stat_recv.at[place],
            device_id={"ep": at_place(q)}, device_id_type=pl.DeviceIdType.MESH,
        )

    def terms_to(q):
        return pltpu.make_async_remote_copy(
            src_ref=msgv.at[at_place(q)], dst_ref=recv.at[place],
            send_sem=send_sem.at[9], recv_sem=recv_sem.at[9],
            device_id={"ep": at_place(q)}, device_id_type=pl.DeviceIdType.MESH,
        )

    def to_those_below(make):
        def step(q, carry):
            make(q).start()
            return carry

        lax.fori_loop(0, place, step, 0)

    to_those_below(statistics_to)
    for copy in loads[1:6]:
        copy.wait()
    gain_here = gain1_v[pl.ds(ep, 1), :]
    gain_high = gain_here.astype(BF16).astype(F32)
    kind = iota((rows8, LANES), 0) % SUB
    centred = (t8 - row_sum * (1.0 / LANES)) * gain_here
    left = jnp.where(
        kind == seq_local, gain_high, jnp.where(kind == seq_local + 1, gain_here - gain_high, centred)
    ).astype(BF16)
    at = 0
    for w in (wv_v, wo_v):
        part = jnp.dot(left, w[...], preferred_element_type=F32)
        for j in range(vt):
            part_s[at] = part[:, j * LANES:(j + 1) * LANES]
            at += 1
    for j in range(2 * vt):
        gain_term = part_s[j, pl.ds(seq_local, 1), :] + part_s[j, pl.ds(seq_local + 1, 1), :]
        term_high = gain_term.astype(BF16).astype(F32)
        part_s[j, pl.ds(seq_local, n_ep, SUB), :] = jnp.broadcast_to(term_high, (n_ep, LANES))
        part_s[j, pl.ds(seq_local + 1, n_ep, SUB), :] = jnp.broadcast_to(
            gain_term - term_high, (n_ep, LANES)
        )
    for p in range(n_ep):
        rows = slice(p * SUB, (p + 1) * SUB)
        for j in range(vt):
            msgv[p, :, j * LANES:(j + 1) * LANES] = jnp.concatenate(
                [part_s[j, rows, :], part_s[vt + j, rows, :]], axis=0
            ).astype(BF16)

    rounds = [1]
    while 2 * rounds[-1] < n_tp // 2:
        rounds.append(2 * rounds[-1])
    to_those_below(terms_to)
    recv[place] = msgv[ep]
    table_up = pltpu.make_async_remote_copy(
        src_ref=table, dst_ref=table, send_sem=send_sem.at[0], recv_sem=recv_sem.at[0],
        device_id={"ep": at_place(place + 2)}, device_id_type=pl.DeviceIdType.MESH,
    )
    tell(known_sem.at[0], rounds[0])

    for copy in loads[6:18]:
        copy.wait()
    here = pl.ds(pl.multiple_of(ep * LANES, LANES), LANES)
    gate_w = jnp.zeros((SUB, LANES), F32)
    for row, source in enumerate((win_v, wfg_v)):
        head = (iota((SUB, n_tp), 1) == tp) & (iota((SUB, n_tp), 0) == row)
        gate_w = gate_w + jnp.dot(head.astype(BF16), source[:, here], preferred_element_type=F32)
    gate_w = gate_w.astype(BF16)
    at_head = iota((1, n_tp), 1) == tp
    input_bias = jnp.sum(jnp.where(at_head, ib_v[...], 0.0), axis=1, keepdims=True)
    forget_bias = jnp.sum(jnp.where(at_head, fb_v[...], 0.0), axis=1, keepdims=True)

    top = routes_v.shape[0]
    own_row = iota((SUB, seqs), 1) == tp * seq_local + iota((SUB, seqs), 0)
    own_row = own_row & (iota((SUB, seqs), 0) < seq_local)
    routed = jnp.zeros((SUB, LANES), F32)
    combine = jnp.zeros((SUB, LANES), F32)
    for k in range(top):
        named = jnp.sum(
            jnp.where(own_row, routes_v[k:k + 1, :].astype(F32) + 1.0, 0.0), axis=1, keepdims=True
        )
        weight = jnp.sum(jnp.where(own_row, rw_v[k:k + 1, :], 0.0), axis=1, keepdims=True)
        match = jnp.abs(named - 1.0 - (lane // SUB).astype(F32)) < 0.5
        routed = routed + jnp.where(match, 1.0, 0.0)
        combine = combine + jnp.where(match, weight, 0.0)
    before = (iota((SUB, SUB), 1) < iota((SUB, SUB), 0)).astype(BF16)
    running = jnp.dot(before, routed.astype(BF16), preferred_element_type=F32)
    placed = jnp.where((routed > 0.5) & (jnp.abs(running - (lane % SUB).astype(F32)) < 0.5), 1.0, 0.0)
    slot_weight = placed * combine
    weight_high = slot_weight.astype(BF16)
    rest = slot_weight - weight_high.astype(F32)
    weight_mid = rest.astype(BF16)
    weight_low = (rest - weight_mid.astype(F32)).astype(BF16)
    capacity = 2
    chosen = [
        jnp.sum(jnp.where(lane == ep * SUB + c, placed, 0.0), axis=1, keepdims=True) for c in range(capacity)
    ]

    if len(rounds) > 1:
        pl.semaphore_wait(known_sem.at[0], 2)
        tell(known_sem.at[1], rounds[1])
    def statistics_from(q):
        pltpu.make_async_copy(rec0.at[q], rec0.at[q], stat_recv.at[q]).wait()

    @pl.when(place < n_ep - 1)
    def _():
        statistics_from(place + 1)
        statistics_to(place + 1).start()
        terms_to(place + 1).start()

    @pl.when(place > 1)
    def _():
        table_up.wait_recv()

    @pl.when(place > 0)
    def _():
        statistics_from(place - 1)
        table[place - 1] = rec0[place - 1]

    table[place] = msg0[...]

    @pl.when(place < n_ep - 2)
    def _():
        statistics_from(place + 2)
        table_up.start()
        terms_to(place + 2).start()

    def from_above(q, carry):
        statistics_from(q)
        terms_to(q).start()
        return carry

    lax.fori_loop(place + 3, n_ep, from_above, 0)
    stat = jnp.zeros((2, rows8), F32)
    for e in range(n_ep):
        theirs = jnp.where(e <= place, table[e], rec0[e])
        stat = stat + theirs
        sum_s[e:e + 1, :] = theirs[0:1]
    stat8 = jnp.where(sub == 0, stat[0:1], jnp.where(sub == 1, stat[1:2], 0.0))
    column = stat8.T
    mean = column[:, 0:1] * (1.0 / features)
    spread = column[:, 1:2] * (1.0 / features) - mean * mean
    normed = ((t8_s[...] - mean) * lax.rsqrt(spread + NORM_EPS) * gain_here).astype(BF16)
    gate_rows = lax.dot_general(gate_w, normed, nt, preferred_element_type=F32)
    for j, w in enumerate((wq_v, wk_v)):
        part = jnp.dot(normed, w[...], preferred_element_type=F32)
        part = jnp.where(kind == seq_local, gate_rows[j:j + 1], part)
        for p in range(n_ep):
            msg1[p, :, j * LANES:(j + 1) * LANES] = part[p * SUB:(p + 1) * SUB]
    q_rows = seq_local + 1
    send(1, "ep", ep_peers, msg1, rec1, True, q_rows)
    rec1[ep] = msg1[ep]

    mine = (lane == ep * SUB + sub) & (sub < seq_local)
    own_mean = jnp.sum(jnp.where(mine, stat[0:1], 0.0), axis=1, keepdims=True) * (1.0 / features)
    own_square = jnp.sum(jnp.where(mine, stat[1:2], 0.0), axis=1, keepdims=True) * (1.0 / features)
    own_inv = lax.rsqrt(own_square - own_mean * own_mean + NORM_EPS)
    off = lax.dot_general(
        jnp.where(mine, 1.0, 0.0), sum_s[...], nt,
        preferred_element_type=F32, precision=lax.Precision.HIGHEST,
    ) * (1.0 / LANES) - own_mean
    if len(rounds) > 2:
        pl.semaphore_wait(known_sem.at[1], 2)
        tell(known_sem.at[2], rounds[2])
    arrive(9, recv)
    for e in range(n_ep):
        arrived = recv[e].astype(F32)
        for j in range(vt):
            piece = arrived[:, j * LANES:(j + 1) * LANES]
            part_s[j, e * SUB:(e + 1) * SUB, :] = piece[:SUB]
            part_s[vt + j, e * SUB:(e + 1) * SUB, :] = piece[SUB:]
    rest_of = []
    for j in range(2 * vt):
        acc = part_s[j, 0:SUB, :]
        for e in range(1, n_ep):
            acc = acc + part_s[j, e * SUB:(e + 1) * SUB, :]
        gain_terms = part_s[j, pl.ds(seq_local, n_ep, SUB), :] + part_s[j, pl.ds(seq_local + 1, n_ep, SUB), :]
        acc = acc + jnp.dot(
            off, gain_terms, preferred_element_type=F32, precision=lax.Precision.HIGHEST
        )
        rest_of.append(jnp.where(sub < seq_local, acc * own_inv, 0.0).astype(BF16).astype(F32))
    value = jnp.concatenate(rest_of[:vt], axis=1)
    outgate = jax.nn.sigmoid(jnp.concatenate(rest_of[vt:], axis=1))
    max8 = jnp.zeros((SUB, LANES), F32)
    for i in range(seq_local):
        max8 = jnp.where(sub == i, max_v[:, i:i + 1], max8)
    head_gain = jnp.concatenate([hg_v[pl.ds(tp * vt + j, 1), :] for j in range(vt)], axis=1)
    wide_p = jnp.concatenate([wp_v[j * LANES:(j + 1) * LANES, :] for j in range(vt)], axis=1)

    arrive(1, rec1, q_rows)
    sums = rec1[0]
    for e in range(1, n_ep):
        sums = sums + rec1[e]
    in8 = jnp.sum(
        jnp.where(mine, sums[seq_local:seq_local + 1, :LANES], 0.0), axis=1, keepdims=True
    ) + input_bias
    fg8 = jnp.sum(
        jnp.where(mine, sums[seq_local:seq_local + 1, LANES:2 * LANES], 0.0), axis=1, keepdims=True
    ) + forget_bias
    carried = jnp.minimum(fg8, 0.0) - jnp.log1p(jnp.exp(-jnp.abs(fg8))) + max8
    new_max = jnp.maximum(carried, in8)
    keep = jnp.exp(carried - new_max)
    admit = jnp.exp(in8 - new_max)
    across = jnp.sum(jnp.where(sub == iota((SUB, LANES), 1), new_max, 0.0), axis=0, keepdims=True)
    nmax_ref[...] = across[:, :seq_local]
    sums = jnp.where(iota((SUB, 2 * LANES), 0) < seq_local, sums, 0.0)
    query = sums[:, :LANES].astype(BF16).astype(F32) * key_size ** (-0.5)
    admitted = admit * sums[:, LANES:2 * LANES].astype(BF16).astype(F32)
    query_t = query.T
    admitted_t = admitted.T
    sub_wide = iota((SUB, value_size), 0)
    readout = jnp.zeros((SUB, value_size), F32)
    for i in range(seq_local):
        nnorm_ref[i] = keep[i:i + 1] * norm_v[i] + admitted[i:i + 1]
        new_cell = keep[i:i + 1, 0:1] * cell_v[i, 0] + admitted_t[:, i:i + 1] * value[i:i + 1, :]
        ncell_ref[i, 0] = new_cell
        read = jnp.sum(query_t[:, i:i + 1] * new_cell, axis=0, keepdims=True)
        readout = jnp.where(sub_wide == i, read, readout)
    head_mean = jnp.mean(readout, axis=1, keepdims=True)
    spread_out = readout - head_mean
    head_var = jnp.mean(spread_out * spread_out, axis=1, keepdims=True)
    mixed = spread_out * lax.rsqrt(head_var + HEAD_EPS) * head_gain * outgate
    mixed = jnp.concatenate([mixed[:, j * LANES:(j + 1) * LANES] for j in range(vt)], axis=0).astype(BF16)
    msg2[...] = mixed

    send(2, "ep", ep_peers, msg2, rec2, False)
    rec2[ep] = mixed
    arrive(2, rec2)
    terms = jnp.dot(
        rec2[...].reshape(n_ep * vt * SUB, LANES), wide_p, preferred_element_type=F32
    )
    for p in range(n_ep):
        term = jnp.zeros((SUB, LANES), F32)
        for j in range(vt):
            start = (p * vt + j) * SUB
            term = term + terms[start:start + SUB, j * LANES:(j + 1) * LANES]
        msg3[p] = term.astype(BF16)
    last = len(rounds) - 1
    pl.semaphore_wait(known_sem.at[last], 2)
    send(3, "tp", tp_peers, msg3, rec3, True, seq_local)
    rec3[tp] = msg3[tp]
    arrive(3, rec3, seq_local)
    mixer = rec3[0].astype(F32)
    for t in range(1, n_tp):
        mixer = mixer + rec3[t].astype(F32)
    mixer = jnp.where(sub < seq_local, mixer, 0.0)
    stream16 = (t8_s[pl.ds(pl.multiple_of(tp * SUB, SUB), SUB), :] + mixer).astype(BF16)
    stream = stream16.astype(F32)
    msg4[...] = stream16

    send(4, "ep", ep_peers, msg4, rec4, False, seq_local)
    rec4[ep] = stream16
    gain2 = gain2_v[...]
    arrive(4, rec4, seq_local)
    for e in range(n_ep):
        slot_s[e * SUB:(e + 1) * SUB, :] = rec4[e].astype(F32)
    rows_of = [slot_s[pl.ds(r, n_ep, SUB), :] for r in range(seq_local)]
    slots = []
    for c in range(capacity):
        x = chosen[c][0:1, :] * rows_of[0]
        for r in range(1, seq_local):
            x = x + chosen[c][r:r + 1, :] * rows_of[r]
        mean = total(x) * (1.0 / features)
        spread = total(x * x) * (1.0 / features) - mean * mean
        slots.append((x - mean) * lax.rsqrt(spread + NORM_EPS) * gain2)
    slots16 = jnp.concatenate(slots, axis=0).astype(BF16)
    msg5[...] = slots16

    send(5, "tp", tp_peers, msg5, rec5, False)
    rec5[tp] = slots16
    for copy in loads[18:]:
        copy.wait()
    arrive(5, rec5)
    rows_c = capacity * n_ep
    slot_count = capacity * n_tp
    for t in range(n_tp):
        wide_s[t * rows_c:(t + 1) * rows_c, :] = rec5[t].astype(F32)
    x = jnp.concatenate(
        [wide_s[pl.ds(e, slot_count, n_ep), :].astype(BF16) for e in range(n_ep)], axis=1
    )
    gate = jnp.dot(x, eg_v[0], preferred_element_type=F32)
    up = jnp.dot(x, eu_v[0], preferred_element_type=F32)
    active = (jax.nn.silu(gate) * up).astype(BF16)
    down = jnp.dot(active, ed_v[0], preferred_element_type=F32)
    for e in range(n_ep):
        wide_s[pl.ds(e, slot_count, n_ep), :] = down[:, e * LANES:(e + 1) * LANES]
    for t in range(n_tp):
        msg6[t] = wide_s[t * rows_c:(t + 1) * rows_c, :].astype(BF16)
    send(6, "tp", tp_peers, msg6, rec6, True)
    rec6[tp] = msg6[tp]
    slot_s[...] = jnp.zeros_like(slot_s)
    arrive(6, rec6)
    done = rec6[0].astype(F32)
    for t in range(1, n_tp):
        done = done + rec6[t].astype(F32)
    for c in range(capacity):
        slot_s[pl.ds(c, n_ep, SUB), :] = done[c * n_ep:(c + 1) * n_ep]
    for e in range(n_ep):
        msg7[e] = slot_s[e * SUB:(e + 1) * SUB, :].astype(BF16)

    send(7, "ep", ep_peers, msg7, rec7, True, capacity)
    rec7[ep] = msg7[ep]
    arrive(7, rec7, capacity)
    returned = jnp.concatenate([rec7[e].astype(F32) for e in range(n_ep)], axis=0).astype(BF16)
    lhs = jnp.concatenate(
        [weight_high.astype(F32), weight_mid.astype(F32), weight_low.astype(F32)], axis=0
    )[:, :SUB * n_ep].astype(BF16)
    moe = jnp.dot(lhs, returned, preferred_element_type=F32)
    moe = moe[0:SUB] + moe[SUB:2 * SUB] + moe[2 * SUB:3 * SUB]
    layer16 = (stream + moe).astype(BF16)
    msg8[...] = layer16
    send(8, "tp", tp_peers, msg8, rec8, False, seq_local)
    rec8[tp] = layer16
    arrive(8, rec8, seq_local)
    finished = jnp.concatenate([rec8[t].astype(F32) for t in range(n_tp)], axis=0).astype(BF16)
    c8 = iota((seqs, SUB * n_tp), 1)
    unpick = (c8 // SUB) * seq_local + c8 % SUB == iota((seqs, SUB * n_tp), 0)
    unpick = unpick & (c8 % SUB < seq_local)
    out_ref[...] = jnp.dot(unpick.astype(BF16), finished, preferred_element_type=F32).astype(BF16)

    @pl.when(place < n_ep - 2)
    def _():
        table_up.wait_send()

    def statistics_left(q, carry):
        pltpu.make_async_copy(msg0, msg0, stat_send.at[q]).wait()
        return carry

    lax.fori_loop(0, place, statistics_left, 0)

    @pl.when(place < n_ep - 1)
    def _():
        statistics_left(place + 1, 0)

    used_rows = (q_rows, None, seq_local, seq_local, None, None, capacity, seq_local, None)
    for phase, target in enumerate((rec1, rec2, rec3, rec4, rec5, rec6, rec7, rec8, recv), 1):
        settle(send_sem.at[phase], target, used_rows[phase - 1])


def write_out(*refs):
    *refs, sem = refs
    count = len(refs) // 2
    copies = [pltpu.make_async_copy(refs[i], refs[count + i], sem.at[i]) for i in range(count)]
    for copy in copies:
        copy.start()
    for copy in copies:
        copy.wait()


def solution(mesh):
    n_ep = mesh.shape["ep"]
    n_tp = mesh.shape["tp"]

    def on_device(*args):
        (
            tokens, first_gain, w_query, w_key, w_value, w_outgate, w_input, w_forget,
            input_bias, forget_bias, head_gain, w_project, cell_state, norm_state, max_state,
            second_gain, routes, route_weight, expert_gate, expert_up, expert_down,
        ) = args
        seq_local = tokens.shape[0] // n_ep
        key_size, value_size = cell_state.shape[2], cell_state.shape[3]
        capacity = 2
        operands = (
            tokens, first_gain.reshape(n_ep, LANES), w_query, w_key, w_value, w_outgate,
            w_input.T, w_forget.T, input_bias.reshape(1, -1), forget_bias.reshape(1, -1),
            head_gain.reshape(-1, LANES), w_project, cell_state, norm_state, max_state.T,
            second_gain.reshape(n_ep, LANES), routes.T, route_weight.T,
            expert_gate, expert_up, expert_down,
        )
        results = (
            jax.ShapeDtypeStruct(tokens.shape, BF16),
            jax.ShapeDtypeStruct(cell_state.shape, F32),
            jax.ShapeDtypeStruct(norm_state.shape, F32),
            jax.ShapeDtypeStruct((1, seq_local), F32),
        )
        hbm = pl.BlockSpec(memory_space=pltpu.HBM)
        vmem = pl.BlockSpec(memory_space=pltpu.VMEM)
        rows8 = max(SUB * n_ep, LANES)
        vt = value_size // LANES

        def pair(shape_out, shape_in, dtype):
            return [pltpu.VMEM(shape_out, dtype), pltpu.VMEM(shape_in, dtype)]

        messages = (
            pair((2, rows8), (n_ep, 2, rows8), F32)
            + pair((n_ep, 2 * SUB, value_size), (n_ep, 2 * SUB, value_size), BF16)
            + pair((n_ep, SUB, 2 * key_size), (n_ep, SUB, 2 * key_size), F32)
            + pair((vt * SUB, LANES), (n_ep, vt * SUB, LANES), BF16)
            + pair((n_tp, SUB, LANES), (n_tp, SUB, LANES), BF16)
            + pair((SUB, LANES), (n_ep, SUB, LANES), BF16)
            + pair((capacity * n_ep, LANES), (n_tp, capacity * n_ep, LANES), BF16)
            + pair((n_tp, capacity * n_ep, LANES), (n_tp, capacity * n_ep, LANES), BF16)
            + pair((n_ep, SUB, LANES), (n_ep, SUB, LANES), BF16)
            + pair((SUB, LANES), (n_tp, SUB, LANES), BF16)
        )
        held = pl.pallas_call(
            functools.partial(kernel, n_ep, n_tp, seq_local, key_size, value_size),
            out_shape=tuple(pltpu.VMEM(r.shape, r.dtype) for r in results),
            in_specs=[hbm] * len(operands),
            out_specs=(vmem, vmem, vmem, vmem),
            scratch_shapes=[pltpu.VMEM(a.shape, a.dtype) for a in operands]
            + messages
            + [
                pltpu.VMEM((n_ep, 2, rows8), F32),
                pltpu.VMEM((rows8, LANES), F32),
                pltpu.VMEM((2 * vt, rows8, LANES), F32),
                pltpu.VMEM((n_ep, rows8), F32),
                pltpu.VMEM((SUB * n_ep, LANES), F32),
                pltpu.VMEM((n_tp * capacity * n_ep, LANES), F32),
                pltpu.SemaphoreType.DMA((len(operands),)),
                pltpu.SemaphoreType.DMA((10,)),
                pltpu.SemaphoreType.DMA((10,)),
                pltpu.SemaphoreType.REGULAR((3,)),
                pltpu.SemaphoreType.DMA((n_ep,)),
                pltpu.SemaphoreType.DMA((n_ep,)),
            ],
            compiler_params=pltpu.CompilerParams(
                collective_id=0, has_side_effects=True
            ),
        )(*operands)
        out, new_cell, new_norm, new_max = pl.pallas_call(
            write_out,
            out_shape=results,
            in_specs=[pl.BlockSpec(memory_space=pl.ANY)] * len(results),
            out_specs=(hbm,) * len(results),
            scratch_shapes=[pltpu.SemaphoreType.DMA((len(results),))],
            compiler_params=pltpu.CompilerParams(vmem_limit_bytes=1024 * 1024),
        )(*held)
        return out, new_cell, new_norm, new_max.T

    placed = (
        P("grp", "ep"), P(), P("ep", "tp"), P("ep", "tp"), P("ep", "tp"), P("ep", "tp"),
        P(), P(), P(), P(), P(), P("tp", "ep"),
        P(("grp", "ep"), "tp", None, None), P(("grp", "ep"), "tp", None), P(("grp", "ep"), "tp"),
        P(), P("grp", None), P("grp", None),
        P("ep", None, "tp"), P("ep", None, "tp"), P("ep", "tp", None),
    )
    return jax.shard_map(
        on_device,
        mesh=mesh,
        in_specs=placed,
        out_specs=(
            P("grp", "ep"),
            P(("grp", "ep"), "tp", None, None),
            P(("grp", "ep"), "tp", None),
            P(("grp", "ep"), "tp"),
        ),
        check_vma=False,
    )
```

```python
import functools

import jax
import jax.numpy as jnp
from jax import lax
from jax.experimental import pallas as pl
from jax.experimental.pallas import tpu as pltpu
from jax.sharding import PartitionSpec as P

NORM_EPS = 1e-05
HEAD_EPS = 1e-06
F32 = jnp.float32
BF16 = jnp.bfloat16
LANES = 128
SUB = 8


def iota(shape, dim):
    return lax.broadcasted_iota(jnp.int32, shape, dim)


def total(x):
    return jnp.sum(jnp.sum(x, axis=1, keepdims=True), axis=0, keepdims=True)


def far_first(n):
    order = [n // 2]
    for d in range(1, n // 2):
        order += [n // 2 + d, n // 2 - d]
    if n % 2 == 0:
        return [d for d in order if 0 < d < n]
    return list(range(1, n))


def kernel(
    n_ep, n_tp, seq_local, key_size, value_size,
    tokens_h, gain1_h, wq_h, wk_h, wv_h, wo_h, win_h, wfg_h, ib_h, fb_h, hg_h, wp_h,
    cell_h, norm_h, max_h, gain2_h, routes_h, rw_h, eg_h, eu_h, ed_h,
    rec8, ncell_ref, nnorm_ref, nmax_ref,
    tokens_v, gain1_v, wq_v, wk_v, wv_v, wo_v, win_v, wfg_v, ib_v, fb_v, hg_v, wp_v,
    cell_v, norm_v, max_v, gain2_v, routes_v, rw_v, eg_v, eu_v, ed_v,
    msg0, rec0, msgv, recv, msg1, rec1, msg2, rec2, msg3, rec3, msg4, rec4, msg5, rec5, msg6, rec6, msg7, rec7, msg8,
    table, t8_s, part_s, sum_s, slot_s, wide_s,
    load_sem, send_sem, recv_sem, known_sem, stat_send, stat_recv,
):
    ep = lax.axis_index("ep")
    tp = lax.axis_index("tp")
    sources = (
        tokens_h, gain1_h, wq_h, wk_h, wv_h, wo_h, win_h, wfg_h, ib_h, fb_h, hg_h, wp_h,
        cell_h, norm_h, max_h, gain2_h, routes_h, rw_h, eg_h, eu_h, ed_h,
    )
    targets = (
        tokens_v, gain1_v, wq_v, wk_v, wv_v, wo_v, win_v, wfg_v, ib_v, fb_v, hg_v, wp_v,
        cell_v, norm_v, max_v, gain2_v, routes_v, rw_v, eg_v, eu_v, ed_v,
    )
    loads = [
        pltpu.make_async_copy(s, t, load_sem.at[i]) for i, (s, t) in enumerate(zip(sources, targets))
    ]
    for copy in loads[:6]:
        copy.start()
    barrier = pltpu.get_barrier_semaphore()
    rec7[...] = jnp.zeros_like(rec7)
    rec8[...] = jnp.zeros_like(rec8)
    table[...] = jnp.zeros_like(table)
    ep_peers = [lax.rem(ep + d, n_ep) for d in far_first(n_ep)]
    tp_peers = [lax.rem(tp + d, n_tp) for d in far_first(n_tp)]
    def ring_tp(r):
        return jnp.where(2 * r < n_tp, 2 * r, 2 * (n_tp - 1 - r) + 1)

    spot = jnp.where(lax.rem(tp, 2) == 0, tp // 2, n_tp - 1 - tp // 2)

    def tell(sem, reach):
        for d in (reach, n_tp - reach):
            peer = ring_tp(lax.rem(spot + d, n_tp))
            pl.semaphore_signal(sem, inc=1, device_id={"tp": peer}, device_id_type=pl.DeviceIdType.MESH)

    tell(barrier, 1)

    place = lax.rem(ep + n_ep - 1, n_ep)

    def at_place(q):
        return lax.rem(q + 1, n_ep)

    @pl.when(place == 0)
    def _():
        pl.semaphore_wait(barrier, 2)

    @pl.when((place > 0) & (place < n_ep - 1))
    def _():
        pl.semaphore_wait(barrier, 3)

    @pl.when(place < n_ep - 1)
    def _():
        pl.semaphore_signal(
            barrier, inc=1, device_id={"ep": at_place(place + 1)}, device_id_type=pl.DeviceIdType.MESH
        )

    def send(phase, axis, peers, source, target, each, used=None):
        me = ep if axis == "ep" else tp
        used = pl.ds(0, target.shape[1] if used is None else used)
        for peer in peers:
            pltpu.make_async_remote_copy(
                src_ref=source.at[peer, used] if each else source.at[used],
                dst_ref=target.at[me, used],
                send_sem=send_sem.at[phase],
                recv_sem=recv_sem.at[phase],
                device_id={axis: peer},
                device_id_type=pl.DeviceIdType.MESH,
            ).start()

    def settle(sem, target, used):
        used = target.shape[1] if used is None else used
        others = target.at[pl.ds(0, target.shape[0] - 1), pl.ds(0, used)]
        pltpu.make_async_copy(others, others, sem).wait()

    def arrive(phase, target, used=None):
        settle(recv_sem.at[phase], target, used)

    rows8 = max(SUB * n_ep, LANES)
    seqs = n_ep * seq_local
    features = n_ep * LANES
    nt = (((1,), (1,)), ((), ()))
    sub = iota((SUB, LANES), 0)
    lane = iota((SUB, LANES), 1)
    kt = key_size // LANES
    vt = value_size // LANES

    loads[0].wait()
    r8 = iota((rows8, seqs), 0)
    pick = ((r8 // SUB) * seq_local + r8 % SUB == iota((rows8, seqs), 1)) & (r8 % SUB < seq_local)
    t8 = jnp.dot(pick.astype(BF16), tokens_v[...], preferred_element_type=F32)
    t8_s[...] = t8
    wide_lane = iota((rows8, LANES), 1)
    row_sum = jnp.sum(t8, axis=1, keepdims=True)
    row_square = jnp.sum(t8 * t8, axis=1, keepdims=True)
    stats = jnp.where(wide_lane == 0, row_sum, jnp.where(wide_lane == 1, row_square, 0.0)).T
    msg0[...] = stats[0:2]

    @pl.when(place == n_ep - 1)
    def _():
        pl.semaphore_wait(barrier, 3)

    def statistics_to(q):
        return pltpu.make_async_remote_copy(
            src_ref=msg0, dst_ref=rec0.at[place], send_sem=stat_send.at[q], recv_sem=stat_recv.at[place],
            device_id={"ep": at_place(q)}, device_id_type=pl.DeviceIdType.MESH,
        )

    def terms_to(q):
        return pltpu.make_async_remote_copy(
            src_ref=msgv.at[at_place(q)], dst_ref=recv.at[place],
            send_sem=send_sem.at[9], recv_sem=recv_sem.at[9],
            device_id={"ep": at_place(q)}, device_id_type=pl.DeviceIdType.MESH,
        )

    def to_those_below(make):
        def step(q, carry):
            make(q).start()
            return carry

        lax.fori_loop(0, place, step, 0)

    to_those_below(statistics_to)
    for copy in loads[6:]:
        copy.start()
    for copy in loads[1:6]:
        copy.wait()
    gain_here = gain1_v[pl.ds(ep, 1), :]
    gain_high = gain_here.astype(BF16).astype(F32)
    kind = iota((rows8, LANES), 0) % SUB
    centred = (t8 - row_sum * (1.0 / LANES)) * gain_here
    left = jnp.where(
        kind == seq_local, gain_high, jnp.where(kind == seq_local + 1, gain_here - gain_high, centred)
    ).astype(BF16)
    at = 0
    for w in (wv_v, wo_v):
        part = jnp.dot(left, w[...], preferred_element_type=F32)
        for j in range(vt):
            part_s[at] = part[:, j * LANES:(j + 1) * LANES]
            at += 1
    for j in range(2 * vt):
        gain_term = part_s[j, pl.ds(seq_local, 1), :] + part_s[j, pl.ds(seq_local + 1, 1), :]
        term_high = gain_term.astype(BF16).astype(F32)
        part_s[j, pl.ds(seq_local, n_ep, SUB), :] = jnp.broadcast_to(term_high, (n_ep, LANES))
        part_s[j, pl.ds(seq_local + 1, n_ep, SUB), :] = jnp.broadcast_to(
            gain_term - term_high, (n_ep, LANES)
        )
    for p in range(n_ep):
        rows = slice(p * SUB, (p + 1) * SUB)
        for j in range(vt):
            msgv[p, :, j * LANES:(j + 1) * LANES] = jnp.concatenate(
                [part_s[j, rows, :], part_s[vt + j, rows, :]], axis=0
            ).astype(BF16)

    rounds = [1]
    while 2 * rounds[-1] < n_tp // 2:
        rounds.append(2 * rounds[-1])
    to_those_below(terms_to)
    recv[place] = msgv[ep]
    table_up = pltpu.make_async_remote_copy(
        src_ref=table, dst_ref=table, send_sem=send_sem.at[0], recv_sem=recv_sem.at[0],
        device_id={"ep": at_place(place + 2)}, device_id_type=pl.DeviceIdType.MESH,
    )
    tell(known_sem.at[0], rounds[0])

    for copy in loads[6:18]:
        copy.wait()
    here = pl.ds(pl.multiple_of(ep * LANES, LANES), LANES)
    gate_w = jnp.zeros((SUB, LANES), F32)
    for row, source in enumerate((win_v, wfg_v)):
        head = (iota((SUB, n_tp), 1) == tp) & (iota((SUB, n_tp), 0) == row)
        gate_w = gate_w + jnp.dot(head.astype(BF16), source[:, here], preferred_element_type=F32)
    gate_w = gate_w.astype(BF16)
    at_head = iota((1, n_tp), 1) == tp
    input_bias = jnp.sum(jnp.where(at_head, ib_v[...], 0.0), axis=1, keepdims=True)
    forget_bias = jnp.sum(jnp.where(at_head, fb_v[...], 0.0), axis=1, keepdims=True)

    top = routes_v.shape[0]
    own_row = iota((SUB, seqs), 1) == tp * seq_local + iota((SUB, seqs), 0)
    own_row = own_row & (iota((SUB, seqs), 0) < seq_local)
    routed = jnp.zeros((SUB, LANES), F32)
    combine = jnp.zeros((SUB, LANES), F32)
    for k in range(top):
        named = jnp.sum(
            jnp.where(own_row, routes_v[k:k + 1, :].astype(F32) + 1.0, 0.0), axis=1, keepdims=True
        )
        weight = jnp.sum(jnp.where(own_row, rw_v[k:k + 1, :], 0.0), axis=1, keepdims=True)
        match = jnp.abs(named - 1.0 - (lane // SUB).astype(F32)) < 0.5
        routed = routed + jnp.where(match, 1.0, 0.0)
        combine = combine + jnp.where(match, weight, 0.0)
    before = (iota((SUB, SUB), 1) < iota((SUB, SUB), 0)).astype(BF16)
    running = jnp.dot(before, routed.astype(BF16), preferred_element_type=F32)
    placed = jnp.where((routed > 0.5) & (jnp.abs(running - (lane % SUB).astype(F32)) < 0.5), 1.0, 0.0)
    slot_weight = placed * combine
    weight_high = slot_weight.astype(BF16)
    rest = slot_weight - weight_high.astype(F32)
    weight_mid = rest.astype(BF16)
    weight_low = (rest - weight_mid.astype(F32)).astype(BF16)
    capacity = 2
    chosen = [
        jnp.sum(jnp.where(lane == ep * SUB + c, placed, 0.0), axis=1, keepdims=True) for c in range(capacity)
    ]

    if len(rounds) > 1:
        pl.semaphore_wait(known_sem.at[0], 2)
        tell(known_sem.at[1], rounds[1])
    def statistics_from(q):
        pltpu.make_async_copy(rec0.at[q], rec0.at[q], stat_recv.at[q]).wait()

    @pl.when(place < n_ep - 1)
    def _():
        statistics_from(place + 1)
        statistics_to(place + 1).start()
        terms_to(place + 1).start()

    @pl.when(place > 1)
    def _():
        table_up.wait_recv()

    @pl.when(place > 0)
    def _():
        statistics_from(place - 1)
        table[place - 1] = rec0[place - 1]

    table[place] = msg0[...]

    @pl.when(place < n_ep - 2)
    def _():
        statistics_from(place + 2)
        table_up.start()
        terms_to(place + 2).start()

    def from_above(q, carry):
        statistics_from(q)
        terms_to(q).start()
        return carry

    lax.fori_loop(place + 3, n_ep, from_above, 0)
    stat = jnp.zeros((2, rows8), F32)
    for e in range(n_ep):
        theirs = jnp.where(e <= place, table[e], rec0[e])
        stat = stat + theirs
        sum_s[e:e + 1, :] = theirs[0:1]
    stat8 = jnp.where(sub == 0, stat[0:1], jnp.where(sub == 1, stat[1:2], 0.0))
    column = stat8.T
    mean = column[:, 0:1] * (1.0 / features)
    spread = column[:, 1:2] * (1.0 / features) - mean * mean
    normed = ((t8_s[...] - mean) * lax.rsqrt(spread + NORM_EPS) * gain_here).astype(BF16)
    gate_rows = lax.dot_general(gate_w, normed, nt, preferred_element_type=F32)
    for j, w in enumerate((wq_v, wk_v)):
        part = jnp.dot(normed, w[...], preferred_element_type=F32)
        part = jnp.where(kind == seq_local, gate_rows[j:j + 1], part)
        for p in range(n_ep):
            msg1[p, :, j * LANES:(j + 1) * LANES] = part[p * SUB:(p + 1) * SUB]
    q_rows = seq_local + 1
    send(1, "ep", ep_peers, msg1, rec1, True, q_rows)
    rec1[ep] = msg1[ep]

    mine = (lane == ep * SUB + sub) & (sub < seq_local)
    own_mean = jnp.sum(jnp.where(mine, stat[0:1], 0.0), axis=1, keepdims=True) * (1.0 / features)
    own_square = jnp.sum(jnp.where(mine, stat[1:2], 0.0), axis=1, keepdims=True) * (1.0 / features)
    own_inv = lax.rsqrt(own_square - own_mean * own_mean + NORM_EPS)
    off = lax.dot_general(
        jnp.where(mine, 1.0, 0.0), sum_s[...], nt,
        preferred_element_type=F32, precision=lax.Precision.HIGHEST,
    ) * (1.0 / LANES) - own_mean
    if len(rounds) > 2:
        pl.semaphore_wait(known_sem.at[1], 2)
        tell(known_sem.at[2], rounds[2])
    arrive(9, recv)
    for e in range(n_ep):
        arrived = recv[e].astype(F32)
        for j in range(vt):
            piece = arrived[:, j * LANES:(j + 1) * LANES]
            part_s[j, e * SUB:(e + 1) * SUB, :] = piece[:SUB]
            part_s[vt + j, e * SUB:(e + 1) * SUB, :] = piece[SUB:]
    rest_of = []
    for j in range(2 * vt):
        acc = part_s[j, 0:SUB, :]
        for e in range(1, n_ep):
            acc = acc + part_s[j, e * SUB:(e + 1) * SUB, :]
        gain_terms = part_s[j, pl.ds(seq_local, n_ep, SUB), :] + part_s[j, pl.ds(seq_local + 1, n_ep, SUB), :]
        acc = acc + jnp.dot(
            off, gain_terms, preferred_element_type=F32, precision=lax.Precision.HIGHEST
        )
        rest_of.append(jnp.where(sub < seq_local, acc * own_inv, 0.0).astype(BF16).astype(F32))
    value = jnp.concatenate(rest_of[:vt], axis=1)
    outgate = jax.nn.sigmoid(jnp.concatenate(rest_of[vt:], axis=1))
    max8 = jnp.zeros((SUB, LANES), F32)
    for i in range(seq_local):
        max8 = jnp.where(sub == i, max_v[:, i:i + 1], max8)
    head_gain = jnp.concatenate([hg_v[pl.ds(tp * vt + j, 1), :] for j in range(vt)], axis=1)
    wide_p = jnp.concatenate([wp_v[j * LANES:(j + 1) * LANES, :] for j in range(vt)], axis=1)

    arrive(1, rec1, q_rows)
    sums = rec1[0]
    for e in range(1, n_ep):
        sums = sums + rec1[e]
    in8 = jnp.sum(
        jnp.where(mine, sums[seq_local:seq_local + 1, :LANES], 0.0), axis=1, keepdims=True
    ) + input_bias
    fg8 = jnp.sum(
        jnp.where(mine, sums[seq_local:seq_local + 1, LANES:2 * LANES], 0.0), axis=1, keepdims=True
    ) + forget_bias
    carried = jnp.minimum(fg8, 0.0) - jnp.log1p(jnp.exp(-jnp.abs(fg8))) + max8
    new_max = jnp.maximum(carried, in8)
    keep = jnp.exp(carried - new_max)
    admit = jnp.exp(in8 - new_max)
    across = jnp.sum(jnp.where(sub == iota((SUB, LANES), 1), new_max, 0.0), axis=0, keepdims=True)
    nmax_ref[...] = across[:, :seq_local]
    sums = jnp.where(iota((SUB, 2 * LANES), 0) < seq_local, sums, 0.0)
    query = sums[:, :LANES].astype(BF16).astype(F32) * key_size ** (-0.5)
    admitted = admit * sums[:, LANES:2 * LANES].astype(BF16).astype(F32)
    query_t = query.T
    admitted_t = admitted.T
    sub_wide = iota((SUB, value_size), 0)
    readout = jnp.zeros((SUB, value_size), F32)
    for i in range(seq_local):
        nnorm_ref[i] = keep[i:i + 1] * norm_v[i] + admitted[i:i + 1]
        new_cell = keep[i:i + 1, 0:1] * cell_v[i, 0] + admitted_t[:, i:i + 1] * value[i:i + 1, :]
        ncell_ref[i, 0] = new_cell
        read = jnp.sum(query_t[:, i:i + 1] * new_cell, axis=0, keepdims=True)
        readout = jnp.where(sub_wide == i, read, readout)
    head_mean = jnp.mean(readout, axis=1, keepdims=True)
    spread_out = readout - head_mean
    head_var = jnp.mean(spread_out * spread_out, axis=1, keepdims=True)
    mixed = spread_out * lax.rsqrt(head_var + HEAD_EPS) * head_gain * outgate
    mixed = jnp.concatenate([mixed[:, j * LANES:(j + 1) * LANES] for j in range(vt)], axis=0).astype(BF16)
    msg2[...] = mixed

    send(2, "ep", ep_peers, msg2, rec2, False)
    rec2[ep] = mixed
    arrive(2, rec2)
    terms = jnp.dot(
        rec2[...].reshape(n_ep * vt * SUB, LANES), wide_p, preferred_element_type=F32
    )
    for p in range(n_ep):
        term = jnp.zeros((SUB, LANES), F32)
        for j in range(vt):
            start = (p * vt + j) * SUB
            term = term + terms[start:start + SUB, j * LANES:(j + 1) * LANES]
        msg3[p] = term.astype(BF16)
    last = len(rounds) - 1
    pl.semaphore_wait(known_sem.at[last], 2)
    send(3, "tp", tp_peers, msg3, rec3, True, seq_local)
    rec3[tp] = msg3[tp]
    arrive(3, rec3, seq_local)
    mixer = rec3[0].astype(F32)
    for t in range(1, n_tp):
        mixer = mixer + rec3[t].astype(F32)
    mixer = jnp.where(sub < seq_local, mixer, 0.0)
    stream16 = (t8_s[pl.ds(pl.multiple_of(tp * SUB, SUB), SUB), :] + mixer).astype(BF16)
    stream = stream16.astype(F32)
    msg4[...] = stream16

    send(4, "ep", ep_peers, msg4, rec4, False, seq_local)
    rec4[ep] = stream16
    gain2 = gain2_v[...]
    arrive(4, rec4, seq_local)
    for e in range(n_ep):
        slot_s[e * SUB:(e + 1) * SUB, :] = rec4[e].astype(F32)
    rows_of = [slot_s[pl.ds(r, n_ep, SUB), :] for r in range(seq_local)]
    slots = []
    for c in range(capacity):
        x = chosen[c][0:1, :] * rows_of[0]
        for r in range(1, seq_local):
            x = x + chosen[c][r:r + 1, :] * rows_of[r]
        mean = total(x) * (1.0 / features)
        spread = total(x * x) * (1.0 / features) - mean * mean
        slots.append((x - mean) * lax.rsqrt(spread + NORM_EPS) * gain2)
    slots16 = jnp.concatenate(slots, axis=0).astype(BF16)
    msg5[...] = slots16

    send(5, "tp", tp_peers, msg5, rec5, False)
    rec5[tp] = slots16
    for copy in loads[18:]:
        copy.wait()
    arrive(5, rec5)
    rows_c = capacity * n_ep
    slot_count = capacity * n_tp
    for t in range(n_tp):
        wide_s[t * rows_c:(t + 1) * rows_c, :] = rec5[t].astype(F32)
    x = jnp.concatenate(
        [wide_s[pl.ds(e, slot_count, n_ep), :].astype(BF16) for e in range(n_ep)], axis=1
    )
    gate = jnp.dot(x, eg_v[0], preferred_element_type=F32)
    up = jnp.dot(x, eu_v[0], preferred_element_type=F32)
    active = (jax.nn.silu(gate) * up).astype(BF16)
    down = jnp.dot(active, ed_v[0], preferred_element_type=F32)
    for e in range(n_ep):
        wide_s[pl.ds(e, slot_count, n_ep), :] = down[:, e * LANES:(e + 1) * LANES]
    for t in range(n_tp):
        msg6[t] = wide_s[t * rows_c:(t + 1) * rows_c, :].astype(BF16)
    send(6, "tp", tp_peers, msg6, rec6, True)
    rec6[tp] = msg6[tp]
    slot_s[...] = jnp.zeros_like(slot_s)
    arrive(6, rec6)
    done = rec6[0].astype(F32)
    for t in range(1, n_tp):
        done = done + rec6[t].astype(F32)
    for c in range(capacity):
        slot_s[pl.ds(c, n_ep, SUB), :] = done[c * n_ep:(c + 1) * n_ep]
    for e in range(n_ep):
        msg7[e] = slot_s[e * SUB:(e + 1) * SUB, :].astype(BF16)

    send(7, "ep", ep_peers, msg7, rec7, True, capacity)
    rec7[ep] = msg7[ep]
    arrive(7, rec7, capacity)
    returned = jnp.concatenate([rec7[e].astype(F32) for e in range(n_ep)], axis=0).astype(BF16)
    lhs = jnp.concatenate(
        [weight_high.astype(F32), weight_mid.astype(F32), weight_low.astype(F32)], axis=0
    )[:, :SUB * n_ep].astype(BF16)
    moe = jnp.dot(lhs, returned, preferred_element_type=F32)
    moe = moe[0:SUB] + moe[SUB:2 * SUB] + moe[2 * SUB:3 * SUB]
    layer16 = (stream + moe).astype(BF16)
    msg8[...] = layer16
    send(8, "tp", tp_peers, msg8, rec8, False, seq_local)
    rec8[tp] = layer16
    arrive(8, rec8, seq_local)
    @pl.when(place < n_ep - 2)
    def _():
        table_up.wait_send()

    def statistics_left(q, carry):
        pltpu.make_async_copy(msg0, msg0, stat_send.at[q]).wait()
        return carry

    lax.fori_loop(0, place, statistics_left, 0)

    @pl.when(place < n_ep - 1)
    def _():
        statistics_left(place + 1, 0)

    used_rows = (q_rows, None, seq_local, seq_local, None, None, capacity, seq_local, None)
    for phase, target in enumerate((rec1, rec2, rec3, rec4, rec5, rec6, rec7, rec8, recv), 1):
        settle(send_sem.at[phase], target, used_rows[phase - 1])


def write_out(seq_local, finished_ref, cell_ref, norm_ref, max_ref, out_h, cell_h, norm_h, max_h, out_v, sem):
    copies = [
        pltpu.make_async_copy(source, target, sem.at[i])
        for i, (source, target) in enumerate(
            ((cell_ref, cell_h), (norm_ref, norm_h), (max_ref, max_h), (out_v, out_h))
        )
    ]
    for copy in copies[:3]:
        copy.start()
    blocks, lanes = finished_ref.shape[0], finished_ref.shape[2]
    finished = jnp.concatenate([finished_ref[t].astype(F32) for t in range(blocks)], axis=0).astype(BF16)
    c8 = iota((out_v.shape[0], SUB * blocks), 1)
    unpick = (c8 // SUB) * seq_local + c8 % SUB == iota(c8.shape, 0)
    unpick = unpick & (c8 % SUB < seq_local)
    out_v[...] = jnp.dot(unpick.astype(BF16), finished, preferred_element_type=F32).astype(BF16)
    copies[3].start()
    for copy in copies:
        copy.wait()


def solution(mesh):
    n_ep = mesh.shape["ep"]
    n_tp = mesh.shape["tp"]

    def on_device(*args):
        (
            tokens, first_gain, w_query, w_key, w_value, w_outgate, w_input, w_forget,
            input_bias, forget_bias, head_gain, w_project, cell_state, norm_state, max_state,
            second_gain, routes, route_weight, expert_gate, expert_up, expert_down,
        ) = args
        seq_local = tokens.shape[0] // n_ep
        key_size, value_size = cell_state.shape[2], cell_state.shape[3]
        capacity = 2
        operands = (
            tokens, first_gain.reshape(n_ep, LANES), w_query, w_key, w_value, w_outgate,
            w_input.T, w_forget.T, input_bias.reshape(1, -1), forget_bias.reshape(1, -1),
            head_gain.reshape(-1, LANES), w_project, cell_state, norm_state, max_state.T,
            second_gain.reshape(n_ep, LANES), routes.T, route_weight.T,
            expert_gate, expert_up, expert_down,
        )
        results = (
            jax.ShapeDtypeStruct(tokens.shape, BF16),
            jax.ShapeDtypeStruct(cell_state.shape, F32),
            jax.ShapeDtypeStruct(norm_state.shape, F32),
            jax.ShapeDtypeStruct((1, seq_local), F32),
        )
        hbm = pl.BlockSpec(memory_space=pltpu.HBM)
        vmem = pl.BlockSpec(memory_space=pltpu.VMEM)
        rows8 = max(SUB * n_ep, LANES)
        vt = value_size // LANES

        def pair(shape_out, shape_in, dtype):
            return [pltpu.VMEM(shape_out, dtype), pltpu.VMEM(shape_in, dtype)]

        messages = (
            pair((2, rows8), (n_ep, 2, rows8), F32)
            + pair((n_ep, 2 * SUB, value_size), (n_ep, 2 * SUB, value_size), BF16)
            + pair((n_ep, SUB, 2 * key_size), (n_ep, SUB, 2 * key_size), F32)
            + pair((vt * SUB, LANES), (n_ep, vt * SUB, LANES), BF16)
            + pair((n_tp, SUB, LANES), (n_tp, SUB, LANES), BF16)
            + pair((SUB, LANES), (n_ep, SUB, LANES), BF16)
            + pair((capacity * n_ep, LANES), (n_tp, capacity * n_ep, LANES), BF16)
            + pair((n_tp, capacity * n_ep, LANES), (n_tp, capacity * n_ep, LANES), BF16)
            + pair((n_ep, SUB, LANES), (n_ep, SUB, LANES), BF16)
            + [pltpu.VMEM((SUB, LANES), BF16)]
        )
        held = pl.pallas_call(
            functools.partial(kernel, n_ep, n_tp, seq_local, key_size, value_size),
            out_shape=(pltpu.VMEM((n_tp, SUB, LANES), BF16),)
            + tuple(pltpu.VMEM(r.shape, r.dtype) for r in results[1:]),
            in_specs=[hbm] * len(operands),
            out_specs=(vmem, vmem, vmem, vmem),
            scratch_shapes=[pltpu.VMEM(a.shape, a.dtype) for a in operands]
            + messages
            + [
                pltpu.VMEM((n_ep, 2, rows8), F32),
                pltpu.VMEM((rows8, LANES), F32),
                pltpu.VMEM((2 * vt, rows8, LANES), F32),
                pltpu.VMEM((n_ep, rows8), F32),
                pltpu.VMEM((SUB * n_ep, LANES), F32),
                pltpu.VMEM((n_tp * capacity * n_ep, LANES), F32),
                pltpu.SemaphoreType.DMA((len(operands),)),
                pltpu.SemaphoreType.DMA((10,)),
                pltpu.SemaphoreType.DMA((10,)),
                pltpu.SemaphoreType.REGULAR((3,)),
                pltpu.SemaphoreType.DMA((n_ep,)),
                pltpu.SemaphoreType.DMA((n_ep,)),
            ],
            compiler_params=pltpu.CompilerParams(
                collective_id=0, has_side_effects=True
            ),
        )(*operands)
        out, new_cell, new_norm, new_max = pl.pallas_call(
            functools.partial(write_out, seq_local),
            out_shape=results,
            in_specs=[vmem] + [pl.BlockSpec(memory_space=pl.ANY)] * 3,
            out_specs=(hbm,) * len(results),
            scratch_shapes=[pltpu.VMEM(tokens.shape, BF16), pltpu.SemaphoreType.DMA((len(results),))],
            compiler_params=pltpu.CompilerParams(vmem_limit_bytes=1024 * 1024),
        )(*held)
        return out, new_cell, new_norm, new_max.T

    placed = (
        P("grp", "ep"), P(), P("ep", "tp"), P("ep", "tp"), P("ep", "tp"), P("ep", "tp"),
        P(), P(), P(), P(), P(), P("tp", "ep"),
        P(("grp", "ep"), "tp", None, None), P(("grp", "ep"), "tp", None), P(("grp", "ep"), "tp"),
        P(), P("grp", None), P("grp", None),
        P("ep", None, "tp"), P("ep", None, "tp"), P("ep", "tp", None),
    )
    return jax.shard_map(
        on_device,
        mesh=mesh,
        in_specs=placed,
        out_specs=(
            P("grp", "ep"),
            P(("grp", "ep"), "tp", None, None),
            P(("grp", "ep"), "tp", None),
            P(("grp", "ep"), "tp"),
        ),
        check_vma=False,
    )
```

```python
import functools

import jax
import jax.numpy as jnp
from jax import lax
from jax.experimental import pallas as pl
from jax.experimental.pallas import tpu as pltpu
from jax.sharding import PartitionSpec as P

NORM_EPS = 1e-05
HEAD_EPS = 1e-06
F32 = jnp.float32
BF16 = jnp.bfloat16
LANES = 128
SUB = 8


def iota(shape, dim):
    return lax.broadcasted_iota(jnp.int32, shape, dim)


def total(x):
    return jnp.sum(jnp.sum(x, axis=1, keepdims=True), axis=0, keepdims=True)


def far_first(n):
    order = [n // 2]
    for d in range(1, n // 2):
        order += [n // 2 + d, n // 2 - d]
    if n % 2 == 0:
        return [d for d in order if 0 < d < n]
    return list(range(1, n))


def kernel(
    n_ep, n_tp, seq_local, key_size, value_size,
    tokens_h, gain1_h, wq_h, wk_h, wv_h, wo_h, win_h, wfg_h, ib_h, fb_h, hg_h, wp_h,
    cell_h, norm_h, max_h, gain2_h, routes_h, rw_h, eg_h, eu_h, ed_h,
    rec8, ncell_ref, nnorm_ref, nmax_ref,
    tokens_v, gain1_v, wq_v, wk_v, wv_v, wo_v, win_v, wfg_v, ib_v, fb_v, hg_v, wp_v,
    cell_v, norm_v, max_v, gain2_v, routes_v, rw_v, eg_v, eu_v, ed_v,
    msg0, rec0, msgv, recv, msg1, rec1, msg2, rec2, msg3, rec3, msg4, rec4, msg5, rec5, msg6, rec6, msg7, rec7, msg8,
    table, t8_s, part_s, sum_s, slot_s, wide_s,
    load_sem, send_sem, recv_sem, known_sem, stat_send, stat_recv,
):
    ep = lax.axis_index("ep")
    tp = lax.axis_index("tp")
    sources = (
        tokens_h, gain1_h, wq_h, wk_h, wv_h, wo_h, win_h, wfg_h, ib_h, fb_h, hg_h, wp_h,
        cell_h, norm_h, max_h, gain2_h, routes_h, rw_h, eg_h, eu_h, ed_h,
    )
    targets = (
        tokens_v, gain1_v, wq_v, wk_v, wv_v, wo_v, win_v, wfg_v, ib_v, fb_v, hg_v, wp_v,
        cell_v, norm_v, max_v, gain2_v, routes_v, rw_v, eg_v, eu_v, ed_v,
    )
    loads = [
        pltpu.make_async_copy(s, t, load_sem.at[i]) for i, (s, t) in enumerate(zip(sources, targets))
    ]
    for copy in loads[:6]:
        copy.start()
    barrier = pltpu.get_barrier_semaphore()
    rec7[...] = jnp.zeros_like(rec7)
    rec8[...] = jnp.zeros_like(rec8)
    table[...] = jnp.zeros_like(table)
    ep_peers = [lax.rem(ep + d, n_ep) for d in far_first(n_ep)]
    tp_peers = [lax.rem(tp + d, n_tp) for d in far_first(n_tp)]
    def tell(sem, reach):
        for d in (reach, n_tp - reach):
            peer = lax.rem(tp + d, n_tp)
            pl.semaphore_signal(sem, inc=1, device_id={"tp": peer}, device_id_type=pl.DeviceIdType.MESH)

    tell(barrier, 1)

    bottom = jnp.where(tp == 0, 1, 0)
    place = lax.rem(ep + n_ep - bottom, n_ep)

    def at_place(q):
        return lax.rem(q + bottom, n_ep)

    @pl.when(place == 0)
    def _():
        pl.semaphore_wait(barrier, 2)

    @pl.when((place > 0) & (place < n_ep - 1))
    def _():
        pl.semaphore_wait(barrier, 3)

    @pl.when(place < n_ep - 1)
    def _():
        pl.semaphore_signal(
            barrier, inc=1, device_id={"ep": at_place(place + 1)}, device_id_type=pl.DeviceIdType.MESH
        )

    def send(phase, axis, peers, source, target, each, used=None):
        me = ep if axis == "ep" else tp
        used = pl.ds(0, target.shape[1] if used is None else used)
        for peer in peers:
            pltpu.make_async_remote_copy(
                src_ref=source.at[peer, used] if each else source.at[used],
                dst_ref=target.at[me, used],
                send_sem=send_sem.at[phase],
                recv_sem=recv_sem.at[phase],
                device_id={axis: peer},
                device_id_type=pl.DeviceIdType.MESH,
            ).start()

    def settle(sem, target, used):
        used = target.shape[1] if used is None else used
        others = target.at[pl.ds(0, target.shape[0] - 1), pl.ds(0, used)]
        pltpu.make_async_copy(others, others, sem).wait()

    def arrive(phase, target, used=None):
        settle(recv_sem.at[phase], target, used)

    rows8 = max(SUB * n_ep, LANES)
    seqs = n_ep * seq_local
    features = n_ep * LANES
    nt = (((1,), (1,)), ((), ()))
    sub = iota((SUB, LANES), 0)
    lane = iota((SUB, LANES), 1)
    kt = key_size // LANES
    vt = value_size // LANES

    loads[0].wait()
    r8 = iota((rows8, seqs), 0)
    pick = ((r8 // SUB) * seq_local + r8 % SUB == iota((rows8, seqs), 1)) & (r8 % SUB < seq_local)
    t8 = jnp.dot(pick.astype(BF16), tokens_v[...], preferred_element_type=F32)
    t8_s[...] = t8
    wide_lane = iota((rows8, LANES), 1)
    row_sum = jnp.sum(t8, axis=1, keepdims=True)
    row_square = jnp.sum(t8 * t8, axis=1, keepdims=True)
    stats = jnp.where(wide_lane == 0, row_sum, jnp.where(wide_lane == 1, row_square, 0.0)).T
    msg0[...] = stats[0:2]

    @pl.when(place == n_ep - 1)
    def _():
        pl.semaphore_wait(barrier, 3)

    def statistics_to(q):
        return pltpu.make_async_remote_copy(
            src_ref=msg0, dst_ref=rec0.at[place], send_sem=stat_send.at[q], recv_sem=stat_recv.at[place],
            device_id={"ep": at_place(q)}, device_id_type=pl.DeviceIdType.MESH,
        )

    def terms_to(q):
        return pltpu.make_async_remote_copy(
            src_ref=msgv.at[at_place(q)], dst_ref=recv.at[place],
            send_sem=send_sem.at[9], recv_sem=recv_sem.at[9],
            device_id={"ep": at_place(q)}, device_id_type=pl.DeviceIdType.MESH,
        )

    def to_those_below(make):
        def step(q, carry):
            make(q).start()
            return carry

        lax.fori_loop(0, place, step, 0)

    to_those_below(statistics_to)
    for copy in loads[6:]:
        copy.start()
    for copy in loads[1:6]:
        copy.wait()
    gain_here = gain1_v[pl.ds(ep, 1), :]
    gain_high = gain_here.astype(BF16).astype(F32)
    kind = iota((rows8, LANES), 0) % SUB
    centred = (t8 - row_sum * (1.0 / LANES)) * gain_here
    left = jnp.where(
        kind == seq_local, gain_high, jnp.where(kind == seq_local + 1, gain_here - gain_high, centred)
    ).astype(BF16)
    at = 0
    for w in (wv_v, wo_v):
        part = jnp.dot(left, w[...], preferred_element_type=F32)
        for j in range(vt):
            part_s[at] = part[:, j * LANES:(j + 1) * LANES]
            at += 1
    for j in range(2 * vt):
        gain_term = part_s[j, pl.ds(seq_local, 1), :] + part_s[j, pl.ds(seq_local + 1, 1), :]
        term_high = gain_term.astype(BF16).astype(F32)
        part_s[j, pl.ds(seq_local, n_ep, SUB), :] = jnp.broadcast_to(term_high, (n_ep, LANES))
        part_s[j, pl.ds(seq_local + 1, n_ep, SUB), :] = jnp.broadcast_to(
            gain_term - term_high, (n_ep, LANES)
        )
    for p in range(n_ep):
        rows = slice(p * SUB, (p + 1) * SUB)
        for j in range(vt):
            msgv[p, :, j * LANES:(j + 1) * LANES] = jnp.concatenate(
                [part_s[j, rows, :], part_s[vt + j, rows, :]], axis=0
            ).astype(BF16)

    rounds = [1]
    while 2 * rounds[-1] < n_tp // 2:
        rounds.append(2 * rounds[-1])
    to_those_below(terms_to)
    recv[place] = msgv[ep]
    table_up = pltpu.make_async_remote_copy(
        src_ref=table, dst_ref=table, send_sem=send_sem.at[0], recv_sem=recv_sem.at[0],
        device_id={"ep": at_place(place + 2)}, device_id_type=pl.DeviceIdType.MESH,
    )
    tell(known_sem.at[0], rounds[0])

    for copy in loads[6:18]:
        copy.wait()
    here = pl.ds(pl.multiple_of(ep * LANES, LANES), LANES)
    gate_w = jnp.zeros((SUB, LANES), F32)
    for row, source in enumerate((win_v, wfg_v)):
        head = (iota((SUB, n_tp), 1) == tp) & (iota((SUB, n_tp), 0) == row)
        gate_w = gate_w + jnp.dot(head.astype(BF16), source[:, here], preferred_element_type=F32)
    gate_w = gate_w.astype(BF16)
    at_head = iota((1, n_tp), 1) == tp
    input_bias = jnp.sum(jnp.where(at_head, ib_v[...], 0.0), axis=1, keepdims=True)
    forget_bias = jnp.sum(jnp.where(at_head, fb_v[...], 0.0), axis=1, keepdims=True)

    top = routes_v.shape[0]
    own_row = iota((SUB, seqs), 1) == tp * seq_local + iota((SUB, seqs), 0)
    own_row = own_row & (iota((SUB, seqs), 0) < seq_local)
    routed = jnp.zeros((SUB, LANES), F32)
    combine = jnp.zeros((SUB, LANES), F32)
    for k in range(top):
        named = jnp.sum(
            jnp.where(own_row, routes_v[k:k + 1, :].astype(F32) + 1.0, 0.0), axis=1, keepdims=True
        )
        weight = jnp.sum(jnp.where(own_row, rw_v[k:k + 1, :], 0.0), axis=1, keepdims=True)
        match = jnp.abs(named - 1.0 - (lane // SUB).astype(F32)) < 0.5
        routed = routed + jnp.where(match, 1.0, 0.0)
        combine = combine + jnp.where(match, weight, 0.0)
    before = (iota((SUB, SUB), 1) < iota((SUB, SUB), 0)).astype(BF16)
    running = jnp.dot(before, routed.astype(BF16), preferred_element_type=F32)
    placed = jnp.where((routed > 0.5) & (jnp.abs(running - (lane % SUB).astype(F32)) < 0.5), 1.0, 0.0)
    slot_weight = placed * combine
    weight_high = slot_weight.astype(BF16)
    rest = slot_weight - weight_high.astype(F32)
    weight_mid = rest.astype(BF16)
    weight_low = (rest - weight_mid.astype(F32)).astype(BF16)
    capacity = 2
    chosen = [
        jnp.sum(jnp.where(lane == ep * SUB + c, placed, 0.0), axis=1, keepdims=True) for c in range(capacity)
    ]

    if len(rounds) > 1:
        pl.semaphore_wait(known_sem.at[0], 2)
        tell(known_sem.at[1], rounds[1])
    def statistics_from(q):
        pltpu.make_async_copy(rec0.at[q], rec0.at[q], stat_recv.at[q]).wait()

    @pl.when(place < n_ep - 1)
    def _():
        statistics_from(place + 1)
        statistics_to(place + 1).start()
        terms_to(place + 1).start()

    @pl.when(place > 1)
    def _():
        table_up.wait_recv()

    @pl.when(place > 0)
    def _():
        statistics_from(place - 1)
        table[place - 1] = rec0[place - 1]

    table[place] = msg0[...]

    @pl.when(place < n_ep - 2)
    def _():
        statistics_from(place + 2)
        table_up.start()
        terms_to(place + 2).start()

    def from_above(q, carry):
        statistics_from(q)
        terms_to(q).start()
        return carry

    lax.fori_loop(place + 3, n_ep, from_above, 0)
    stat = jnp.zeros((2, rows8), F32)
    for e in range(n_ep):
        theirs = jnp.where(e <= place, table[e], rec0[e])
        stat = stat + theirs
        sum_s[e:e + 1, :] = theirs[0:1]
    stat8 = jnp.where(sub == 0, stat[0:1], jnp.where(sub == 1, stat[1:2], 0.0))
    column = stat8.T
    mean = column[:, 0:1] * (1.0 / features)
    spread = column[:, 1:2] * (1.0 / features) - mean * mean
    normed = ((t8_s[...] - mean) * lax.rsqrt(spread + NORM_EPS) * gain_here).astype(BF16)
    gate_rows = lax.dot_general(gate_w, normed, nt, preferred_element_type=F32)
    for j, w in enumerate((wq_v, wk_v)):
        part = jnp.dot(normed, w[...], preferred_element_type=F32)
        part = jnp.where(kind == seq_local, gate_rows[j:j + 1], part)
        for p in range(n_ep):
            msg1[p, :, j * LANES:(j + 1) * LANES] = part[p * SUB:(p + 1) * SUB]
    q_rows = seq_local + 1
    send(1, "ep", ep_peers, msg1, rec1, True, q_rows)
    rec1[ep] = msg1[ep]

    mine = (lane == ep * SUB + sub) & (sub < seq_local)
    own_mean = jnp.sum(jnp.where(mine, stat[0:1], 0.0), axis=1, keepdims=True) * (1.0 / features)
    own_square = jnp.sum(jnp.where(mine, stat[1:2], 0.0), axis=1, keepdims=True) * (1.0 / features)
    own_inv = lax.rsqrt(own_square - own_mean * own_mean + NORM_EPS)
    off = lax.dot_general(
        jnp.where(mine, 1.0, 0.0), sum_s[...], nt,
        preferred_element_type=F32, precision=lax.Precision.HIGHEST,
    ) * (1.0 / LANES) - own_mean
    if len(rounds) > 2:
        pl.semaphore_wait(known_sem.at[1], 2)
        tell(known_sem.at[2], rounds[2])
    arrive(9, recv)
    for e in range(n_ep):
        arrived = recv[e].astype(F32)
        for j in range(vt):
            piece = arrived[:, j * LANES:(j + 1) * LANES]
            part_s[j, e * SUB:(e + 1) * SUB, :] = piece[:SUB]
            part_s[vt + j, e * SUB:(e + 1) * SUB, :] = piece[SUB:]
    rest_of = []
    for j in range(2 * vt):
        acc = part_s[j, 0:SUB, :]
        for e in range(1, n_ep):
            acc = acc + part_s[j, e * SUB:(e + 1) * SUB, :]
        gain_terms = part_s[j, pl.ds(seq_local, n_ep, SUB), :] + part_s[j, pl.ds(seq_local + 1, n_ep, SUB), :]
        acc = acc + jnp.dot(
            off, gain_terms, preferred_element_type=F32, precision=lax.Precision.HIGHEST
        )
        rest_of.append(jnp.where(sub < seq_local, acc * own_inv, 0.0).astype(BF16).astype(F32))
    value = jnp.concatenate(rest_of[:vt], axis=1)
    outgate = jax.nn.sigmoid(jnp.concatenate(rest_of[vt:], axis=1))
    max8 = jnp.zeros((SUB, LANES), F32)
    for i in range(seq_local):
        max8 = jnp.where(sub == i, max_v[:, i:i + 1], max8)
    head_gain = jnp.concatenate([hg_v[pl.ds(tp * vt + j, 1), :] for j in range(vt)], axis=1)
    wide_p = jnp.concatenate([wp_v[j * LANES:(j + 1) * LANES, :] for j in range(vt)], axis=1)

    arrive(1, rec1, q_rows)
    sums = rec1[0]
    for e in range(1, n_ep):
        sums = sums + rec1[e]
    in8 = jnp.sum(
        jnp.where(mine, sums[seq_local:seq_local + 1, :LANES], 0.0), axis=1, keepdims=True
    ) + input_bias
    fg8 = jnp.sum(
        jnp.where(mine, sums[seq_local:seq_local + 1, LANES:2 * LANES], 0.0), axis=1, keepdims=True
    ) + forget_bias
    carried = jnp.minimum(fg8, 0.0) - jnp.log1p(jnp.exp(-jnp.abs(fg8))) + max8
    new_max = jnp.maximum(carried, in8)
    keep = jnp.exp(carried - new_max)
    admit = jnp.exp(in8 - new_max)
    across = jnp.sum(jnp.where(sub == iota((SUB, LANES), 1), new_max, 0.0), axis=0, keepdims=True)
    nmax_ref[...] = across[:, :seq_local]
    sums = jnp.where(iota((SUB, 2 * LANES), 0) < seq_local, sums, 0.0)
    query = sums[:, :LANES].astype(BF16).astype(F32) * key_size ** (-0.5)
    admitted = admit * sums[:, LANES:2 * LANES].astype(BF16).astype(F32)
    query_t = query.T
    admitted_t = admitted.T
    sub_wide = iota((SUB, value_size), 0)
    readout = jnp.zeros((SUB, value_size), F32)
    for i in range(seq_local):
        nnorm_ref[i] = keep[i:i + 1] * norm_v[i] + admitted[i:i + 1]
        new_cell = keep[i:i + 1, 0:1] * cell_v[i, 0] + admitted_t[:, i:i + 1] * value[i:i + 1, :]
        ncell_ref[i, 0] = new_cell
        read = jnp.sum(query_t[:, i:i + 1] * new_cell, axis=0, keepdims=True)
        readout = jnp.where(sub_wide == i, read, readout)
    head_mean = jnp.mean(readout, axis=1, keepdims=True)
    spread_out = readout - head_mean
    head_var = jnp.mean(spread_out * spread_out, axis=1, keepdims=True)
    mixed = spread_out * lax.rsqrt(head_var + HEAD_EPS) * head_gain * outgate
    mixed = jnp.concatenate([mixed[:, j * LANES:(j + 1) * LANES] for j in range(vt)], axis=0).astype(BF16)
    msg2[...] = mixed

    send(2, "ep", ep_peers, msg2, rec2, False)
    rec2[ep] = mixed
    arrive(2, rec2)
    terms = jnp.dot(
        rec2[...].reshape(n_ep * vt * SUB, LANES), wide_p, preferred_element_type=F32
    )
    for p in range(n_ep):
        term = jnp.zeros((SUB, LANES), F32)
        for j in range(vt):
            start = (p * vt + j) * SUB
            term = term + terms[start:start + SUB, j * LANES:(j + 1) * LANES]
        msg3[p] = term.astype(BF16)
    last = len(rounds) - 1
    pl.semaphore_wait(known_sem.at[last], 2)
    send(3, "tp", tp_peers, msg3, rec3, True, seq_local)
    rec3[tp] = msg3[tp]
    arrive(3, rec3, seq_local)
    mixer = rec3[0].astype(F32)
    for t in range(1, n_tp):
        mixer = mixer + rec3[t].astype(F32)
    mixer = jnp.where(sub < seq_local, mixer, 0.0)
    stream16 = (t8_s[pl.ds(pl.multiple_of(tp * SUB, SUB), SUB), :] + mixer).astype(BF16)
    stream = stream16.astype(F32)
    msg4[...] = stream16

    send(4, "ep", ep_peers, msg4, rec4, False, seq_local)
    rec4[ep] = stream16
    gain2 = gain2_v[...]
    arrive(4, rec4, seq_local)
    for e in range(n_ep):
        slot_s[e * SUB:(e + 1) * SUB, :] = rec4[e].astype(F32)
    rows_of = [slot_s[pl.ds(r, n_ep, SUB), :] for r in range(seq_local)]
    slots = []
    for c in range(capacity):
        x = chosen[c][0:1, :] * rows_of[0]
        for r in range(1, seq_local):
            x = x + chosen[c][r:r + 1, :] * rows_of[r]
        mean = total(x) * (1.0 / features)
        spread = total(x * x) * (1.0 / features) - mean * mean
        slots.append((x - mean) * lax.rsqrt(spread + NORM_EPS) * gain2)
    slots16 = jnp.concatenate(slots, axis=0).astype(BF16)
    msg5[...] = slots16

    send(5, "tp", tp_peers, msg5, rec5, False)
    rec5[tp] = slots16
    for copy in loads[18:]:
        copy.wait()
    arrive(5, rec5)
    rows_c = capacity * n_ep
    slot_count = capacity * n_tp
    for t in range(n_tp):
        wide_s[t * rows_c:(t + 1) * rows_c, :] = rec5[t].astype(F32)
    x = jnp.concatenate(
        [wide_s[pl.ds(e, slot_count, n_ep), :].astype(BF16) for e in range(n_ep)], axis=1
    )
    gate = jnp.dot(x, eg_v[0], preferred_element_type=F32)
    up = jnp.dot(x, eu_v[0], preferred_element_type=F32)
    active = (jax.nn.silu(gate) * up).astype(BF16)
    down = jnp.dot(active, ed_v[0], preferred_element_type=F32)
    for e in range(n_ep):
        wide_s[pl.ds(e, slot_count, n_ep), :] = down[:, e * LANES:(e + 1) * LANES]
    for t in range(n_tp):
        msg6[t] = wide_s[t * rows_c:(t + 1) * rows_c, :].astype(BF16)
    send(6, "tp", tp_peers, msg6, rec6, True)
    rec6[tp] = msg6[tp]
    slot_s[...] = jnp.zeros_like(slot_s)
    arrive(6, rec6)
    done = rec6[0].astype(F32)
    for t in range(1, n_tp):
        done = done + rec6[t].astype(F32)
    for c in range(capacity):
        slot_s[pl.ds(c, n_ep, SUB), :] = done[c * n_ep:(c + 1) * n_ep]
    for e in range(n_ep):
        msg7[e] = slot_s[e * SUB:(e + 1) * SUB, :].astype(BF16)

    send(7, "ep", ep_peers, msg7, rec7, True, capacity)
    rec7[ep] = msg7[ep]
    arrive(7, rec7, capacity)
    returned = jnp.concatenate([rec7[e].astype(F32) for e in range(n_ep)], axis=0).astype(BF16)
    lhs = jnp.concatenate(
        [weight_high.astype(F32), weight_mid.astype(F32), weight_low.astype(F32)], axis=0
    )[:, :SUB * n_ep].astype(BF16)
    moe = jnp.dot(lhs, returned, preferred_element_type=F32)
    moe = moe[0:SUB] + moe[SUB:2 * SUB] + moe[2 * SUB:3 * SUB]
    layer16 = (stream + moe).astype(BF16)
    msg8[...] = layer16
    send(8, "tp", tp_peers, msg8, rec8, False, seq_local)
    rec8[tp] = layer16
    arrive(8, rec8, seq_local)
    @pl.when(place < n_ep - 2)
    def _():
        table_up.wait_send()

    def statistics_left(q, carry):
        pltpu.make_async_copy(msg0, msg0, stat_send.at[q]).wait()
        return carry

    lax.fori_loop(0, place, statistics_left, 0)

    @pl.when(place < n_ep - 1)
    def _():
        statistics_left(place + 1, 0)

    used_rows = (q_rows, None, seq_local, seq_local, None, None, capacity, seq_local, None)
    for phase, target in enumerate((rec1, rec2, rec3, rec4, rec5, rec6, rec7, rec8, recv), 1):
        settle(send_sem.at[phase], target, used_rows[phase - 1])


def write_out(seq_local, finished_ref, cell_ref, norm_ref, max_ref, out_h, cell_h, norm_h, max_h, out_v, sem):
    copies = [
        pltpu.make_async_copy(source, target, sem.at[i])
        for i, (source, target) in enumerate(
            ((cell_ref, cell_h), (norm_ref, norm_h), (max_ref, max_h), (out_v, out_h))
        )
    ]
    for copy in copies[:3]:
        copy.start()
    blocks, lanes = finished_ref.shape[0], finished_ref.shape[2]
    finished = jnp.concatenate([finished_ref[t].astype(F32) for t in range(blocks)], axis=0).astype(BF16)
    c8 = iota((out_v.shape[0], SUB * blocks), 1)
    unpick = (c8 // SUB) * seq_local + c8 % SUB == iota(c8.shape, 0)
    unpick = unpick & (c8 % SUB < seq_local)
    out_v[...] = jnp.dot(unpick.astype(BF16), finished, preferred_element_type=F32).astype(BF16)
    copies[3].start()
    for copy in copies:
        copy.wait()


def solution(mesh):
    n_ep = mesh.shape["ep"]
    n_tp = mesh.shape["tp"]

    def on_device(*args):
        (
            tokens, first_gain, w_query, w_key, w_value, w_outgate, w_input, w_forget,
            input_bias, forget_bias, head_gain, w_project, cell_state, norm_state, max_state,
            second_gain, routes, route_weight, expert_gate, expert_up, expert_down,
        ) = args
        seq_local = tokens.shape[0] // n_ep
        key_size, value_size = cell_state.shape[2], cell_state.shape[3]
        capacity = 2
        operands = (
            tokens, first_gain.reshape(n_ep, LANES), w_query, w_key, w_value, w_outgate,
            w_input.T, w_forget.T, input_bias.reshape(1, -1), forget_bias.reshape(1, -1),
            head_gain.reshape(-1, LANES), w_project, cell_state, norm_state, max_state.T,
            second_gain.reshape(n_ep, LANES), routes.T, route_weight.T,
            expert_gate, expert_up, expert_down,
        )
        results = (
            jax.ShapeDtypeStruct(tokens.shape, BF16),
            jax.ShapeDtypeStruct(cell_state.shape, F32),
            jax.ShapeDtypeStruct(norm_state.shape, F32),
            jax.ShapeDtypeStruct((1, seq_local), F32),
        )
        hbm = pl.BlockSpec(memory_space=pltpu.HBM)
        vmem = pl.BlockSpec(memory_space=pltpu.VMEM)
        rows8 = max(SUB * n_ep, LANES)
        vt = value_size // LANES

        def pair(shape_out, shape_in, dtype):
            return [pltpu.VMEM(shape_out, dtype), pltpu.VMEM(shape_in, dtype)]

        messages = (
            pair((2, rows8), (n_ep, 2, rows8), F32)
            + pair((n_ep, 2 * SUB, value_size), (n_ep, 2 * SUB, value_size), BF16)
            + pair((n_ep, SUB, 2 * key_size), (n_ep, SUB, 2 * key_size), F32)
            + pair((vt * SUB, LANES), (n_ep, vt * SUB, LANES), BF16)
            + pair((n_tp, SUB, LANES), (n_tp, SUB, LANES), BF16)
            + pair((SUB, LANES), (n_ep, SUB, LANES), BF16)
            + pair((capacity * n_ep, LANES), (n_tp, capacity * n_ep, LANES), BF16)
            + pair((n_tp, capacity * n_ep, LANES), (n_tp, capacity * n_ep, LANES), BF16)
            + pair((n_ep, SUB, LANES), (n_ep, SUB, LANES), BF16)
            + [pltpu.VMEM((SUB, LANES), BF16)]
        )
        held = pl.pallas_call(
            functools.partial(kernel, n_ep, n_tp, seq_local, key_size, value_size),
            out_shape=(pltpu.VMEM((n_tp, SUB, LANES), BF16),)
            + tuple(pltpu.VMEM(r.shape, r.dtype) for r in results[1:]),
            in_specs=[hbm] * len(operands),
            out_specs=(vmem, vmem, vmem, vmem),
            scratch_shapes=[pltpu.VMEM(a.shape, a.dtype) for a in operands]
            + messages
            + [
                pltpu.VMEM((n_ep, 2, rows8), F32),
                pltpu.VMEM((rows8, LANES), F32),
                pltpu.VMEM((2 * vt, rows8, LANES), F32),
                pltpu.VMEM((n_ep, rows8), F32),
                pltpu.VMEM((SUB * n_ep, LANES), F32),
                pltpu.VMEM((n_tp * capacity * n_ep, LANES), F32),
                pltpu.SemaphoreType.DMA((len(operands),)),
                pltpu.SemaphoreType.DMA((10,)),
                pltpu.SemaphoreType.DMA((10,)),
                pltpu.SemaphoreType.REGULAR((3,)),
                pltpu.SemaphoreType.DMA((n_ep,)),
                pltpu.SemaphoreType.DMA((n_ep,)),
            ],
            compiler_params=pltpu.CompilerParams(
                collective_id=0, has_side_effects=True
            ),
        )(*operands)
        out, new_cell, new_norm, new_max = pl.pallas_call(
            functools.partial(write_out, seq_local),
            out_shape=results,
            in_specs=[vmem] + [pl.BlockSpec(memory_space=pl.ANY)] * 3,
            out_specs=(hbm,) * len(results),
            scratch_shapes=[pltpu.VMEM(tokens.shape, BF16), pltpu.SemaphoreType.DMA((len(results),))],
            compiler_params=pltpu.CompilerParams(vmem_limit_bytes=1024 * 1024),
        )(*held)
        return out, new_cell, new_norm, new_max.T

    placed = (
        P("grp", "ep"), P(), P("ep", "tp"), P("ep", "tp"), P("ep", "tp"), P("ep", "tp"),
        P(), P(), P(), P(), P(), P("tp", "ep"),
        P(("grp", "ep"), "tp", None, None), P(("grp", "ep"), "tp", None), P(("grp", "ep"), "tp"),
        P(), P("grp", None), P("grp", None),
        P("ep", None, "tp"), P("ep", None, "tp"), P("ep", "tp", None),
    )
    return jax.shard_map(
        on_device,
        mesh=mesh,
        in_specs=placed,
        out_specs=(
            P("grp", "ep"),
            P(("grp", "ep"), "tp", None, None),
            P(("grp", "ep"), "tp", None),
            P(("grp", "ep"), "tp"),
        ),
        check_vma=False,
    )
```
